32 devices in a mesh: ep: 8 (over z, x), tp: 4 (over y, core).
Axes of the slice: x: 2, y: 2, z: 4, core: 2. Of those that a mesh axis runs over, the one named last changes fastest.
Arguments:
- queries: bfloat16 [4096, 1024], P('ep', 'tp'), may hold values from -6 to 6
- key_input: bfloat16 [4096, 256], P('ep'), may hold values from -6 to 6
- value_input: bfloat16 [4096, 256], P('ep'), may hold values from -6 to 6
- query_gain: float32 [64], replicated, may hold values from 0.1 to 1.9
- key_gain: float32 [64], replicated, may hold values from 0.1 to 1.9
- mix_out_weight: bfloat16 [1024, 2048], P('tp'), may hold values from -0.1875 to 0.1875
- expert_input: bfloat16 [1280, 2048], P('ep'), may hold values from -6 to 6
- ffn_gain: float32 [2048], replicated, may hold values from 0.1 to 1.9
- routes: int32 [1280, 2], P('ep'), may hold values from 0 to 7, all different within a row; in each aligned block of 160 rows (0 to 159, 160 to 319, ...) at most 60 rows name the same one
- route_scores: float32 [1280, 2], P('ep'), may hold values from 0.1 to 1
- gate_weight: bfloat16 [8, 2048, 4096], P('ep', None, 'tp'), may hold values from -0.125 to 0.125
- up_weight: bfloat16 [8, 2048, 4096], P('ep', None, 'tp'), may hold values from -0.125 to 0.125
- down_weight: bfloat16 [8, 4096, 2048], P('ep', 'tp'), may hold values from -0.09375 to 0.09375
Outputs:
- mixed_rows: bfloat16 [4096, 2048], P(('ep', 'tp'))
- expert_out: bfloat16 [1280, 2048], P('ep', 'tp')
The draws below stay inside these ranges and needn't reach their ends.
Inputs may be any that keep to these rules, and one draw needn't show every extreme that they name: `routes`: each row names 2 different experts. Within the rows of one index of ep (aligned blocks of 160 rows) no expert is named by more than 60 rows, and in every draw some expert is named by exactly 60 rows of some block.
All inputs are finite; a program needn't handle non-finite values.
Results may differ from the reference program's by a relative error of at most 0.019.
The reference program's roundings to bfloat16 on the way count: a program that leaves them out, or rounds other values in their place, can miss the bound.
Values may be sent and summed in bfloat16 or wider, within the bound.
No kernel may reach another device: no remote copies, remote signals or barrier semaphores. Data moves between devices by JAX's collectives and lax.ppermute only.
A program may use at most 64 MiB of HBM per device.

```python
import math
import jax
import jax.numpy as jnp
import numpy as np
from jax import lax

D = 2048
HEADS = 16
KV_HEADS = 4
HD = 64
GRID_W = 64
FF = 4096
TOPK = 2
TOK2 = 160
EXPERTS = 8
CAP = 60
TOKENS1 = 4096
TOKENS2 = 1280
N_EP = 8
N_TP = 4


def block_levels(rng, dims, shards, least, top_value):
    loudness = 1.0
    for dim, parts in shards:
        heights = jax.random.uniform(jax.random.fold_in(jax.random.fold_in(rng, 6), dim), (parts,), jnp.float32, least / len(shards), top_value / len(shards))
        loudness = loudness * jnp.repeat(jnp.exp(heights), dims[dim] // parts).reshape((-1,) + (1,) * (len(dims) - 1 - dim))
    return loudness


def routed_block(stream_key, own, number, rows, number_of, top, most, skew):
    order = jax.random.permutation(stream_key, number_of)
    crowded, usual = portions_of(number_of, rows * top, most, skew, True), portions_of(number_of, rows * top, most, skew, False)
    places = jnp.arange(number_of)

    def named(tallies, rotation):
        used = int((tallies > 0).sum())
        fixed = max(1, used // 4)
        passed = fixed + (places - fixed + rotation * (used - fixed)) % max(1, number_of - fixed)
        return jnp.zeros((number_of,), jnp.int32).at[order[jnp.where(places < fixed, places, passed)]].set(jnp.asarray(tallies, jnp.int32))

    tallies = jnp.where(number % 4 == 0, named(crowded, number // 4), named(usual, number - number // 4 - 1))
    mixed = jax.random.permutation(jax.random.fold_in(own, 3), number_of)
    donor, taker = mixed[0:number_of // 2 * 2:2], mixed[1:number_of // 2 * 2:2]
    margin = jnp.minimum(tallies[donor] - 1, most - tallies[taker]) // 2
    margin = jnp.where((donor == order[0]) | (taker == order[0]) | (tallies[taker] == 0), 0, jnp.maximum(margin, 0))
    passed = jax.random.randint(jax.random.fold_in(own, 4), (number_of // 2,), 0, 1 << 20) % (margin + 1)
    tallies = tallies.at[donor].add(-passed).at[taker].add(passed)
    items = jnp.searchsorted(jnp.cumsum(tallies), jnp.arange(rows * top), side="right").astype(jnp.int32)
    listing = items.reshape(top, rows).T
    listing = listing[jax.random.permutation(jax.random.fold_in(own, 1), rows)]
    rotation = jax.random.randint(jax.random.fold_in(own, 2), (rows, 1), 0, top)
    return jnp.take_along_axis(listing, (jnp.arange(top)[None, :] + rotation) % top, axis=1)


def portions_of(count, total, bound, skew, full):
    loads = [(1 << 20) // math.isqrt(rank ** skew) + 1 for rank in range(1, count + 1)]
    largest = bound if full else min(bound, max(-(-total // count), total * loads[0] // sum(loads)))
    least = 1 if total - largest >= count - 1 else 0
    given, spare = [largest] + [least] * (count - 1), total - largest - least * (count - 1)
    while spare > 0:
        movable = [i for i in range(1, count) if given[i] < largest] or [i for i in range(1, count) if given[i] < bound]
        whole, budget = sum([loads[i] for i in movable]), spare
        for i in movable:
            more = min(bound - given[i], max(1, budget * loads[i] // whole), spare)
            given[i] = given[i] + more
            spare = spare - more
    return np.array(given)


def noise(key, extent, deviation, bound, cuts=(), kind=jnp.bfloat16):
    factor_of = block_levels(key, extent, cuts, -0.22, 0.18) if cuts else 1.0
    array = jax.random.normal(key, extent, jnp.float32) * deviation * factor_of
    return jnp.minimum(jnp.maximum(array, -bound), bound).astype(kind)


def setup_inputs(seed: int = 0) -> dict:
    streams_of = jax.random.split(jax.random.key(seed), 14)
    queries = noise(streams_of[0], (TOKENS1, HEADS * HD), 1.0, 6.0, ((0, 8), (1, 4)))
    key_input = noise(streams_of[1], (TOKENS1, KV_HEADS * HD), 1.0, 6.0, ((0, 8),))
    value_input = noise(streams_of[2], (TOKENS1, KV_HEADS * HD), 1.0, 6.0, ((0, 8),))
    query_gain = jnp.clip(1.0 + 0.18 * jax.random.normal(streams_of[3], (HD,), jnp.float32), 0.1, 1.9)
    key_gain = jnp.clip(1.0 + 0.18 * jax.random.normal(streams_of[4], (HD,), jnp.float32), 0.1, 1.9)
    mix_out_weight = noise(streams_of[5], (HEADS * HD, D), (HEADS * HD) ** -0.5, 0.1875, ((0, 4),))
    expert_input = noise(streams_of[6], (TOKENS2, D), 1.0, 6.0, ((0, 8),))
    ffn_gain = jnp.clip(1.0 + 0.18 * jax.random.normal(streams_of[7], (D,), jnp.float32), 0.1, 1.9)
    routes_keys = jax.random.split(jax.random.fold_in(streams_of[8], 1), TOKENS2 // TOK2)
    routes_turns = jax.random.permutation(jax.random.fold_in(streams_of[8], 3), TOKENS2 // TOK2)
    routes = jax.vmap(lambda own, number: routed_block(jax.random.fold_in(streams_of[8], 2), own, number, TOK2, EXPERTS, TOPK, CAP, 2))(routes_keys, routes_turns).reshape((TOKENS2, TOPK))
    route_scores = jnp.clip(jnp.exp(math.log(1.0) - 2.3025851 * jax.random.uniform(streams_of[9], (TOKENS2, TOPK), jnp.float32) ** block_levels(streams_of[9], (TOKENS2, TOPK), ((0, 8),), -0.2, 0.2)), 0.1, 1.0)
    gate_weight = noise(streams_of[10], (EXPERTS, D, FF), D ** -0.5, 0.125, ((0, 8), (2, 4)))
    up_weight = noise(streams_of[11], (EXPERTS, D, FF), D ** -0.5, 0.125, ((0, 8), (2, 4)))
    down_weight = noise(streams_of[12], (EXPERTS, FF, D), FF ** -0.5, 0.09375, ((0, 8), (1, 4)))
    return dict(queries=queries, key_input=key_input, value_input=value_input, query_gain=query_gain, key_gain=key_gain, mix_out_weight=mix_out_weight, expert_input=expert_input, ffn_gain=ffn_gain, routes=routes, route_scores=route_scores, gate_weight=gate_weight, up_weight=up_weight, down_weight=down_weight)


EPSILON = 1e-06
ROPE_BASE = 10000.0

def rotate_half(portion, cos_table, sin_table):
    front_half, back_half = jnp.split(portion, 2, axis=-1)
    cos_table = cos_table[:, None, :]
    sin_table = sin_table[:, None, :]
    return jnp.concatenate([front_half * cos_table - back_half * sin_table, back_half * cos_table + front_half * sin_table], axis=-1)

def prepare(source, channel_gain, positions):
    token_count = source.shape[0]
    values_f = source.astype(jnp.float32).reshape(token_count, -1, HD)
    normed = values_f * lax.rsqrt(lax.optimization_barrier(jnp.mean(values_f * values_f, axis=-1, keepdims=True)) + EPSILON) * channel_gain
    quarter = HD // 4
    inverse = ROPE_BASE ** (-jnp.arange(quarter, dtype=jnp.float32) / quarter)
    row_angle = (positions // GRID_W).astype(jnp.float32)[:, None] * inverse[None, :]
    col_angle = (positions % GRID_W).astype(jnp.float32)[:, None] * inverse[None, :]
    half_width = HD // 2
    turned = jnp.concatenate([rotate_half(normed[..., :half_width], jnp.cos(row_angle), jnp.sin(row_angle)), rotate_half(normed[..., half_width:], jnp.cos(col_angle), jnp.sin(col_angle))], axis=-1)
    return turned.reshape(token_count, -1).astype(jnp.bfloat16)

def attend_head(head_args):
    query_head, key_head, value_head = head_args
    length = query_head.shape[0]
    key_span = math.gcd(length, 512)
    query_blocks = query_head.reshape(length // key_span, key_span, HD)

    def one_block(query_block):
        scores = jnp.dot(query_block, key_head.T, preferred_element_type=jnp.float32) * HD ** (-0.5)
        weights = jnp.exp(scores)
        weighted = jnp.dot(weights.astype(jnp.bfloat16), value_head, preferred_element_type=jnp.float32)
        return (weighted / lax.optimization_barrier(jnp.sum(weights, axis=-1, keepdims=True))).astype(jnp.bfloat16)
    return lax.map(one_block, query_blocks).reshape(length, HD)

def reference(queries, key_input, value_input, query_gain, key_gain, mix_out_weight, expert_input, ffn_gain, routes, route_scores, gate_weight, up_weight, down_weight):
    length = queries.shape[0]
    positions = jnp.arange(length, dtype=jnp.int32)
    group_size = HEADS // KV_HEADS
    q_rot = prepare(queries, query_gain, positions).reshape(length, HEADS, HD).transpose(1, 0, 2)
    k_rot = prepare(key_input, key_gain, positions).reshape(length, KV_HEADS, HD).transpose(1, 0, 2)
    v_heads = value_input.reshape(length, KV_HEADS, HD).transpose(1, 0, 2)
    attended = lax.map(attend_head, (q_rot, jnp.repeat(k_rot, group_size, axis=0), jnp.repeat(v_heads, group_size, axis=0)))
    attended = attended.transpose(1, 0, 2).reshape(length, HEADS * HD)
    col_width = HEADS * HD // N_TP

    def add_group(running_sum, group_index):
        start_col = (group_index * col_width).astype(jnp.int32)
        columns = lax.dynamic_slice_in_dim(attended, start_col, col_width, 1)
        weight_rows = lax.dynamic_slice_in_dim(mix_out_weight, start_col, col_width, 0)
        portion = jnp.dot(columns, weight_rows, preferred_element_type=jnp.float32).astype(jnp.bfloat16)
        portion = lax.optimization_barrier(portion)
        return (running_sum + portion.astype(jnp.float32), None)
    mixed_sum, _ = lax.scan(add_group, jnp.zeros((length, D), jnp.float32), jnp.arange(N_TP, dtype=jnp.int32))
    mixed_rows = mixed_sum.astype(jnp.bfloat16)
    tokens = expert_input.shape[0]
    flat_routes = routes.reshape(N_EP, TOK2 * TOPK)
    hit_table = (flat_routes[:, :, None] == jnp.arange(EXPERTS, dtype=jnp.int32)[None, None, :]).astype(jnp.int32)
    position = lax.optimization_barrier(jnp.sum((jnp.cumsum(hit_table, axis=1) - hit_table) * hit_table, axis=-1))
    per_expert = N_EP * CAP
    slot_index = flat_routes * per_expert + jnp.arange(N_EP, dtype=jnp.int32)[:, None] * CAP + position
    slot_index = slot_index.reshape(-1).astype(jnp.int32)
    pair_token = jnp.arange(tokens * TOPK, dtype=jnp.int32) // TOPK
    owner_row = jnp.full((EXPERTS * per_expert,), tokens, jnp.int32).at[slot_index].set(pair_token)
    padded = jnp.concatenate([expert_input, jnp.zeros((1, D), jnp.bfloat16)], axis=0)
    buffers = padded[owner_row].reshape(EXPERTS, per_expert, D)
    ff_width = FF // N_TP

    def run_expert(expert_args):
        slot_rows, w_gate, w_up, w_down = expert_args
        values_f = slot_rows.astype(jnp.float32)
        row_scale = lax.rsqrt(lax.optimization_barrier(jnp.mean(values_f * values_f, axis=-1, keepdims=True)) + EPSILON)
        scaled = (values_f * ffn_gain).astype(jnp.bfloat16)
        gate_pre = row_scale * jnp.dot(scaled, w_gate, preferred_element_type=jnp.float32)
        up_pre = row_scale * jnp.dot(scaled, w_up, preferred_element_type=jnp.float32)
        hidden = (jax.nn.silu(gate_pre) * up_pre).astype(jnp.bfloat16)
        running_sum = jnp.zeros((per_expert, D), jnp.float32)
        for group_index in range(N_TP):
            lower = group_index * ff_width
            portion = jnp.dot(hidden[:, lower:lower + ff_width], w_down[lower:lower + ff_width], preferred_element_type=jnp.float32).astype(jnp.bfloat16)
            running_sum = running_sum + lax.optimization_barrier(portion).astype(jnp.float32)
        return running_sum.astype(jnp.bfloat16)
    pair_rows = lax.map(run_expert, (buffers, gate_weight, up_weight, down_weight)).reshape(-1, D)
    route_weight = route_scores / lax.optimization_barrier(jnp.sum(route_scores, axis=-1, keepdims=True))
    picked = pair_rows[slot_index].astype(jnp.float32).reshape(tokens, TOPK, D)
    expert_out = lax.optimization_barrier(jnp.sum(picked * route_weight[:, :, None], axis=1)).astype(jnp.bfloat16)
    return (mixed_rows, expert_out)
```

```python
import functools

import jax
import jax.numpy as jnp
import numpy as np
from jax import lax
from jax.experimental import pallas as pl
from jax.experimental.pallas import tpu as pltpu
from jax.sharding import PartitionSpec as P

HEADS = 16
KV_HEADS = 4
HD = 64
GRID_W = 64
EPSILON = 1e-06
ROPE_BASE = 10000.0
LOG2E = 1.4426950408889634
F32 = jnp.float32
BF16 = jnp.bfloat16
VMEM_LIMIT = 48 * 1024 * 1024
CHUNKS = 1


def full(shape):
    return pl.BlockSpec(shape, lambda *_: (0,) * len(shape))


def call(body, name, place, args, in_specs, outs, grid=(1,), scratch=(), out_specs=None):
    return pl.pallas_call(
        body,
        name=name,
        grid_spec=pltpu.PrefetchScalarGridSpec(
            num_scalar_prefetch=1,
            grid=grid,
            in_specs=in_specs,
            out_specs=[full(o.shape) for o in outs] if out_specs is None else out_specs,
            scratch_shapes=list(scratch),
        ),
        out_shape=outs,
        compiler_params=pltpu.CompilerParams(
            dimension_semantics=("arbitrary",) * len(grid), vmem_limit_bytes=VMEM_LIMIT
        ),
    )(place, *args)


def mm(a, b, dims=((1,), (0,))):
    return lax.dot_general(a, b, (dims, ((), ())), preferred_element_type=F32)


def send(x, axis, flip):
    n = lax.axis_size(axis)
    return lax.ppermute(x, axis, [(i, i ^ flip) for i in range(n)])


def dispatch_body(place, routes_ref, x_ref, *outs, experts, cap, chunks):
    out_refs, sidx_ref = outs[:chunks], outs[chunks]
    tokens = x_ref.shape[0]
    routes = routes_ref[...]
    lanes = lax.broadcasted_iota(jnp.int32, (tokens, 128), 1)
    first = (lanes == routes[:, 0:1]).astype(F32)
    second = (lanes == routes[:, 1:2]).astype(F32)
    hits = (first + second).astype(BF16)
    row = lax.broadcasted_iota(jnp.int32, (tokens, tokens), 0)
    col = lax.broadcasted_iota(jnp.int32, (tokens, tokens), 1)
    before = (row < col).astype(F32).astype(BF16)
    eye = (row == col).astype(F32).astype(BF16)
    after = (row > col).astype(F32).astype(BF16)
    hits_t = mm(hits, eye, ((0,), (0,)))
    count_t = mm(hits, before, ((0,), (0,)))
    slot_t = jnp.where(hits_t > 0.5, count_t, -1.0).astype(jnp.int32)
    count = mm(after, hits)
    x = x_ref[...]
    part = cap // chunks
    for c in range(chunks):
        slots = lax.broadcasted_iota(jnp.int32, (part, tokens), 0) + c * part
        for e in range(experts):
            pick = (slots == slot_t[e : e + 1, :]).astype(F32).astype(BF16)
            out_refs[c][e * part : (e + 1) * part, :] = mm(pick, x).astype(BF16)
    slot0 = jnp.sum(count * first, axis=1, keepdims=True).astype(jnp.int32)
    slot1 = jnp.sum(count * second, axis=1, keepdims=True).astype(jnp.int32)

    def flat(slot, expert):
        piece = sum([(slot >= c * part).astype(jnp.int32) for c in range(1, chunks)], jnp.zeros_like(slot))
        return piece * (experts * part) + expert * part + slot - piece * part

    sidx_ref[...] = jnp.where(
        lanes == 0, flat(slot0, routes[:, 0:1]), jnp.where(lanes == 1, flat(slot1, routes[:, 1:2]), 0)
    )


def dispatch(place, routes, expert_input, experts, cap, chunks, feat):
    tokens = routes.shape[0]
    outs = [jax.ShapeDtypeStruct((experts * cap // chunks, feat), BF16)] * chunks
    outs += [jax.ShapeDtypeStruct((tokens, 128), jnp.int32)]
    return call(
        functools.partial(dispatch_body, experts=experts, cap=cap, chunks=chunks),
        "dispatch",
        place,
        (routes, expert_input),
        [full(routes.shape), pl.BlockSpec((tokens, feat), lambda i, place: (0, place[0]))],
        outs,
    )


def rope_tables(token_count, n_ep):
    quarter = HD // 4
    inverse = (np.float32(ROPE_BASE) ** (-np.arange(quarter, dtype=np.float32) / np.float32(quarter))).astype(
        np.float32
    )
    pos = np.arange(token_count * n_ep)

    def both(steps):
        angle = (inverse[:, None] * steps.astype(np.float32)[None, :]).astype(np.float32).astype(np.float64)
        return np.concatenate([np.cos(angle), np.sin(angle)], 0).astype(np.float32)

    return np.concatenate([both(pos // GRID_W), both(pos % GRID_W)], 0)


def turn(x, gain, table, low):
    quarter = HD // 4
    x = x.astype(F32)
    scale = lax.rsqrt(jnp.mean(x * x, axis=0, keepdims=True) + EPSILON)
    x = x * scale * gain
    u0, w0, u1, w1 = (x[i * quarter : (i + 1) * quarter] for i in range(4))
    cr, sr, cc, sc = (table[i * quarter : (i + 1) * quarter] for i in range(4))
    return jnp.concatenate(
        [u0 * cr - w0 * sr, w0 * cr + u0 * sr, u1 * cc - w1 * sc, w1 * cc + u1 * sc], axis=0
    ).astype(low)


def prep_body(place, q_ref, k_ref, v_ref, gains_ref, table_ref, qt_ref, kvt_ref, turned_ref, *, heads, group):
    table = table_ref[...]
    gains = gains_ref[...]
    q_gain = gains[:, 0:1]
    k_gain = gains[:, 1:2]
    qt = q_ref[...].astype(F32).T
    for h in range(heads):
        qt_ref[h * HD : (h + 1) * HD, :] = turn(qt[h * HD : (h + 1) * HD], q_gain, table, BF16)
    start = pl.multiple_of((place[0] * heads // group) * HD, HD)
    turned_ref[...] = k_ref[...].astype(F32).T
    kvt_ref[:HD, :] = turn(turned_ref[pl.ds(start, HD), :], k_gain, table, BF16)
    turned_ref[...] = v_ref[...].astype(F32).T
    kvt_ref[HD:, :] = turned_ref[pl.ds(start, HD), :].astype(BF16)


def prep(place, queries, key_input, value_input, gains, table, heads):
    rows = queries.shape[0]
    return call(
        functools.partial(prep_body, heads=heads, group=HEADS // KV_HEADS),
        "prep",
        place,
        (queries, key_input, value_input, gains, table),
        [
            full(queries.shape),
            full(key_input.shape),
            full(value_input.shape),
            full(gains.shape),
            pl.BlockSpec((table.shape[0], rows), lambda i, place: (0, place[1])),
        ],
        [
            jax.ShapeDtypeStruct((queries.shape[1], rows), BF16),
            jax.ShapeDtypeStruct((2 * HD, rows), BF16),
        ],
        scratch=[pltpu.VMEM((key_input.shape[1], rows), F32)],
    )


def attend_body(place, qt_ref, *refs, blocks, heads):
    kv_refs, out_ref, k_ref, v_ref, num_ref, den_ref = refs[:blocks], *refs[blocks:]
    keys = kv_refs[0].shape[1]
    for b in range(blocks):
        k_ref[b] = kv_refs[b][:HD, :].astype(F32).T.astype(BF16)
        v_ref[b] = kv_refs[b][HD:, :]
    num_ref[...] = jnp.zeros_like(num_ref)
    den_ref[...] = jnp.zeros_like(den_ref)

    def one(b, carry):
        k = k_ref[b]
        v = v_ref[b]
        for h in range(heads):
            q = qt_ref[h * HD : (h + 1) * HD, :]
            p = jnp.exp2(mm(k, q) * (LOG2E * HD**-0.5))
            den_ref[h * 8 : (h + 1) * 8, :] += jnp.sum(p.reshape(keys // 8, 8, p.shape[1]), axis=0)
            num_ref[h * HD : (h + 1) * HD, :] += mm(v, p.astype(BF16))
        return carry

    lax.fori_loop(0, blocks, one, 0)
    for h in range(heads):
        den = jnp.sum(den_ref[h * 8 : (h + 1) * 8, :], axis=0, keepdims=True)
        num_ref[h * HD : (h + 1) * HD, :] = num_ref[h * HD : (h + 1) * HD, :] / den
    out_ref[...] = num_ref[...].T.astype(BF16)


def attend(place, qt, kv_blocks, heads):
    rows = qt.shape[1]
    keys = kv_blocks[0].shape[1]
    blocks = len(kv_blocks)
    return call(
        functools.partial(attend_body, blocks=blocks, heads=heads),
        "attend",
        place,
        (qt, *kv_blocks),
        [full(qt.shape)] + [full(b.shape) for b in kv_blocks],
        [jax.ShapeDtypeStruct((rows, qt.shape[0]), BF16)],
        scratch=[
            pltpu.VMEM((blocks, keys, HD), BF16),
            pltpu.VMEM((blocks, HD, keys), BF16),
            pltpu.VMEM(qt.shape, F32),
            pltpu.VMEM((heads * 8, rows), F32),
        ],
    )[0]


def mix_body(place, att_ref, *refs, groups):
    w_refs, out_ref = refs[:groups], refs[groups]
    rows = out_ref.shape[0]
    total = jnp.zeros(out_ref.shape, F32)
    for k in range(groups):
        at = pl.multiple_of((place[0] ^ k) * rows, rows)
        total += mm(att_ref[pl.ds(at, rows), :], w_refs[k][...]).astype(BF16).astype(F32)
    out_ref[...] = total.astype(BF16)


def mix(place, att, weights):
    groups = len(weights)
    rows = att.shape[0] // groups
    width = weights[0].shape[1]
    return call(
        functools.partial(mix_body, groups=groups),
        "mix",
        place,
        (att, *weights),
        [full(att.shape)] + [full(w.shape) for w in weights],
        [jax.ShapeDtypeStruct((rows, width), BF16)],
    )[0]


def expert_body(place, *refs, groups, steps):
    x_refs = refs[:groups]
    gain_ref, gate_ref, up_ref, down_ref = refs[groups : groups + 4]
    out_refs = refs[groups + 4 : 2 * groups + 4]
    scaled_ref, rms_ref, acc_ref = refs[2 * groups + 4 :]
    feat = x_refs[0].shape[1]
    width = groups * feat
    step = pl.program_id(0)

    def origin(k):
        return place[0] ^ k

    @pl.when(step == 0)
    def _():
        squares = 0.0
        for k in range(groups):
            x = x_refs[k][...].astype(F32)
            scaled_ref[k] = (x * gain_ref[pl.ds(origin(k), 1), :]).astype(BF16)
            squares += jnp.sum(x * x, axis=1, keepdims=True)
        rms_ref[...] = jnp.broadcast_to(lax.rsqrt(squares / width + EPSILON), rms_ref.shape)

    gate = 0.0
    up = 0.0
    for k in range(groups):
        rows = pl.ds(pl.multiple_of(origin(k) * feat, feat), feat)
        gate += mm(scaled_ref[k], gate_ref[0, rows, :])
        up += mm(scaled_ref[k], up_ref[0, rows, :])
    scale = rms_ref[:, 0:1]
    gate = gate * scale
    hidden = (gate / (1.0 + jnp.exp(-gate)) * (up * scale)).astype(BF16)
    for k in range(groups):
        cols = pl.ds(pl.multiple_of(origin(k) * feat, feat), feat)
        part = mm(hidden, down_ref[0, :, cols])
        if steps == 1:
            out_refs[k][...] = part.astype(BF16)
        else:

            @pl.when(step == 0)
            def _():
                acc_ref[k] = part

            @pl.when((step > 0) & (step < steps - 1))
            def _():
                acc_ref[k] += part

            @pl.when(step == steps - 1)
            def _():
                out_refs[k][...] = (acc_ref[k] + part).astype(BF16)


def expert(place, xs, gain, gate, up, down):
    groups = len(xs)
    rows, feat = xs[0].shape
    ff = gate.shape[2]
    depth = gate.shape[1]
    tile = min(ff, 256)
    steps = ff // tile
    return call(
        functools.partial(expert_body, groups=groups, steps=steps),
        "expert",
        place,
        (*xs, gain, gate, up, down),
        [full(x.shape) for x in xs]
        + [
            full(gain.shape),
            pl.BlockSpec((1, depth, tile), lambda j, place: (0, 0, j)),
            pl.BlockSpec((1, depth, tile), lambda j, place: (0, 0, j)),
            pl.BlockSpec((1, tile, depth), lambda j, place: (0, j, 0)),
        ],
        [jax.ShapeDtypeStruct((rows, feat), BF16)] * groups,
        grid=(steps,),
        scratch=[
            pltpu.VMEM((groups, rows, feat), BF16),
            pltpu.VMEM((rows, 128), F32),
            pltpu.VMEM((groups, rows, feat), F32),
        ],
    )


def combine_body(place, sidx_ref, scores_ref, *refs, chunks):
    row_refs, out_ref = refs[:chunks], refs[chunks]
    tokens = out_ref.shape[0]
    slots = row_refs[0].shape[0]
    scores = scores_ref[...]
    weight = scores / jnp.sum(scores, axis=1, keepdims=True)
    sidx = sidx_ref[...]
    total = jnp.zeros(out_ref.shape, F32)
    for k in range(2):
        picked = jnp.zeros(out_ref.shape, F32)
        for c in range(chunks):
            lanes = lax.broadcasted_iota(jnp.int32, (tokens, slots), 1) + c * slots
            pick = (lanes == sidx[:, k : k + 1]).astype(F32).astype(BF16)
            picked += mm(pick, row_refs[c][...])
        total += picked * weight[:, k : k + 1]
    out_ref[...] = total.astype(BF16)


def combine(place, sidx, scores, rows):
    return call(
        functools.partial(combine_body, chunks=len(rows)),
        "combine",
        place,
        (sidx, scores, *rows),
        [full(sidx.shape), full(scores.shape)] + [full(r.shape) for r in rows],
        [jax.ShapeDtypeStruct((sidx.shape[0], rows[0].shape[1]), BF16)],
    )[0]


def local(
    table,
    queries,
    key_input,
    value_input,
    query_gain,
    key_gain,
    mix_out_weight,
    expert_input,
    ffn_gain,
    routes,
    route_scores,
    gate_weight,
    up_weight,
    down_weight,
):
    n_ep = lax.axis_size("ep")
    n_tp = lax.axis_size("tp")
    heads = queries.shape[1] // HD
    tokens, top = routes.shape
    width = expert_input.shape[1]
    feat = width // n_tp
    cap = 3 * tokens * top // (2 * n_ep)
    unit = 8 * CHUNKS
    cap = -(-cap // unit) * unit
    place = jnp.stack([lax.axis_index("tp"), lax.axis_index("ep")]).astype(jnp.int32)

    *outbound, sidx = dispatch(place, routes, expert_input, n_ep, cap, CHUNKS, feat)
    arrived = [lax.all_to_all(o, "ep", split_axis=0, concat_axis=0, tiled=True) for o in outbound]

    gains = jnp.stack([query_gain, key_gain], axis=1)
    qt, kvt = prep(place, queries, key_input, value_input, gains, table, heads)
    blocks = [kvt] + [send(kvt, "ep", k) for k in range(2, n_ep, 2)]
    blocks += [send(b, "ep", 1) for b in blocks]

    weights = {0: mix_out_weight}
    for k in range(2, n_tp, 2):
        weights[k] = send(mix_out_weight, "tp", k)
    for k in range(0, n_tp, 2):
        weights[k + 1] = send(weights[k], "tp", 1)

    gain = ffn_gain.reshape(n_tp, feat)
    reduced = []
    for a in arrived:
        xs = {0: a}
        for k in range(2, n_tp, 2):
            xs[k] = send(a, "tp", k)
        for k in range(0, n_tp, 2):
            xs[k + 1] = send(xs[k], "tp", 1)
        parts = expert(place, [xs[k] for k in range(n_tp)], gain, gate_weight, up_weight, down_weight)
        pairs = {}
        for k in range(0, n_tp, 2):
            pairs[k] = parts[k].astype(F32) + send(parts[k + 1], "tp", 1).astype(F32)
        total = pairs[0]
        for k in range(2, n_tp, 2):
            total += send(pairs[k].astype(BF16), "tp", k).astype(F32)
        reduced.append(total.astype(BF16))

    att = attend(place, qt, blocks, heads)
    att = lax.all_to_all(att, "tp", split_axis=0, concat_axis=0, tiled=True)
    mixed = mix(place, att, [weights[k] for k in range(n_tp)])

    returned = [lax.all_to_all(r, "ep", split_axis=0, concat_axis=0, tiled=True) for r in reduced]
    out = combine(place, sidx, route_scores, returned)
    return mixed, out


def solution(mesh):
    n_ep = mesh.shape["ep"]
    placed = (
        P(),
        P("ep", "tp"),
        P("ep", None),
        P("ep", None),
        P(),
        P(),
        P("tp", None),
        P("ep", None),
        P(),
        P("ep", None),
        P("ep", None),
        P("ep", None, "tp"),
        P("ep", None, "tp"),
        P("ep", "tp", None),
    )
    step = jax.shard_map(
        local,
        mesh=mesh,
        in_specs=placed,
        out_specs=(P(("ep", "tp"), None), P("ep", "tp")),
        check_vma=False,
    )

    def run(queries, *rest):
        table = jnp.asarray(rope_tables(queries.shape[0] // n_ep, n_ep))
        return step(table, queries, *rest)

    return run
```

```python
import functools

import jax
import jax.numpy as jnp
import numpy as np
from jax import lax
from jax.experimental import pallas as pl
from jax.experimental.pallas import tpu as pltpu
from jax.sharding import PartitionSpec as P


HEADS = 16
KV_HEADS = 4
HD = 64
GRID_W = 64
EPSILON = 1e-06
ROPE_BASE = 10000.0
LOG2E = 1.4426950408889634
F32 = jnp.float32
BF16 = jnp.bfloat16
VMEM_LIMIT = 48 * 1024 * 1024
FLOPS_PER_MICRO = 500_000_000
CHUNKS = 1


def full(shape):
    return pl.BlockSpec(shape, lambda *_: (0,) * len(shape))


def hbm():
    return pl.BlockSpec(memory_space=pltpu.HBM)


def call(body, place, args, in_specs, outs, grid=(1,), scratch=(), out_specs=None, micros=1.0):
    return pl.pallas_call(
        body,
        grid_spec=pltpu.PrefetchScalarGridSpec(
            num_scalar_prefetch=1,
            grid=grid,
            in_specs=in_specs,
            out_specs=[full(o.shape) for o in outs] if out_specs is None else out_specs,
            scratch_shapes=list(scratch),
        ),
        out_shape=outs,
        cost_estimate=pl.CostEstimate(
            flops=int(micros * FLOPS_PER_MICRO), transcendentals=0, bytes_accessed=0
        ),
        compiler_params=pltpu.CompilerParams(
            dimension_semantics=("arbitrary",) * len(grid), vmem_limit_bytes=VMEM_LIMIT
        ),
    )(place, *args)


def mm(a, b, dims=((1,), (0,))):
    return lax.dot_general(a, b, (dims, ((), ())), preferred_element_type=F32)


def send(x, axis, flip):
    n = lax.axis_size(axis)
    return lax.ppermute(x, axis, [(i, i ^ flip) for i in range(n)])


def dispatch_body(place, routes_ref, x_hbm, *outs, experts, cap, chunks):
    out_refs, slot_ref, x_ref, sem = outs[:chunks], *outs[chunks:]
    tokens, feat = x_ref.shape
    cols = pl.ds(pl.multiple_of(place[0] * feat, feat), feat)
    fetch = pltpu.make_async_copy(x_hbm.at[:, cols], x_ref, sem)
    fetch.start()
    routes = routes_ref[...]
    rows = lax.broadcasted_iota(jnp.int32, (experts, tokens), 0)
    first = (rows == routes[0:1, :]).astype(F32)
    second = (rows == routes[1:2, :]).astype(F32)
    hits = first + second
    row = lax.broadcasted_iota(jnp.int32, (tokens, tokens), 0)
    col = lax.broadcasted_iota(jnp.int32, (tokens, tokens), 1)
    before = (row < col).astype(F32).astype(BF16)
    count = mm(hits.astype(BF16), before)
    slot = jnp.where(hits > 0.5, count, -1.0).astype(jnp.int32)
    part = cap // chunks

    def flat(choice, expert):
        at = jnp.sum(count * choice, axis=0, keepdims=True).astype(jnp.int32)
        piece = sum([(at >= c * part).astype(jnp.int32) for c in range(1, chunks)], jnp.zeros_like(at))
        return piece * (experts * part) + expert * part + at - piece * part

    slot_ref[0:1, :] = flat(first, routes[0:1, :])
    slot_ref[1:2, :] = flat(second, routes[1:2, :])
    fetch.wait()
    x = x_ref[...]
    for c in range(chunks):
        slots = lax.broadcasted_iota(jnp.int32, (part, tokens), 0) + c * part
        for e in range(experts):
            pick = (slots == slot[e : e + 1, :]).astype(F32).astype(BF16)
            out_refs[c][e * part : (e + 1) * part, :] = mm(pick, x).astype(BF16)


def dispatch(place, routes, expert_input, experts, cap, chunks, feat):
    tokens = routes.shape[1]
    outs = [jax.ShapeDtypeStruct((experts * cap // chunks, feat), BF16)] * chunks
    outs += [jax.ShapeDtypeStruct((2, tokens), jnp.int32)]
    return call(
        functools.partial(dispatch_body, experts=experts, cap=cap, chunks=chunks),
        place,
        (routes, expert_input),
        [full(routes.shape), hbm()],
        outs,
        scratch=[pltpu.VMEM((tokens, feat), BF16), pltpu.SemaphoreType.DMA],
        micros=1.5,
    )


def rope_tables(token_count, n_ep):
    quarter = HD // 4
    inverse = (np.float32(ROPE_BASE) ** (-np.arange(quarter, dtype=np.float32) / np.float32(quarter))).astype(
        np.float32
    )
    pos = np.arange(token_count * n_ep)

    def both(steps):
        angle = (inverse[:, None] * steps.astype(np.float32)[None, :]).astype(np.float32).astype(np.float64)
        return np.concatenate([np.cos(angle), np.sin(angle)], 0).astype(np.float32)

    return np.concatenate([both(pos // GRID_W), both(pos % GRID_W)], 0)


def turn(x, gain, table, low):
    quarter = HD // 4
    x = x.astype(F32)
    scale = lax.rsqrt(jnp.mean(x * x, axis=0, keepdims=True) + EPSILON)
    x = x * scale * gain
    u0, w0, u1, w1 = (x[i * quarter : (i + 1) * quarter] for i in range(4))
    cr, sr, cc, sc = (table[i * quarter : (i + 1) * quarter] for i in range(4))
    return jnp.concatenate(
        [u0 * cr - w0 * sr, w0 * cr + u0 * sr, u1 * cc - w1 * sc, w1 * cc + u1 * sc], axis=0
    ).astype(low)


def column(row):
    n = row.shape[1]
    same = lax.broadcasted_iota(jnp.int32, (n, n), 0) == lax.broadcasted_iota(jnp.int32, (n, n), 1)
    return jnp.sum(jnp.where(same, row, 0.0), axis=1, keepdims=True)


def prep_body(
    place, q_ref, k_ref, v_ref, q_gain_ref, k_gain_ref, table_ref, qt_ref, kvt_ref, turned_ref, *, heads, group
):
    table = table_ref[...]
    q_gain = column(q_gain_ref[...])
    k_gain = column(k_gain_ref[...])
    qt = q_ref[...].astype(F32).T
    for h in range(heads):
        qt_ref[h * HD : (h + 1) * HD, :] = turn(qt[h * HD : (h + 1) * HD], q_gain, table, BF16)
    start = pl.multiple_of((place[0] * heads // group) * HD, HD)
    turned_ref[...] = k_ref[...].astype(F32).T
    kvt_ref[:HD, :] = turn(turned_ref[pl.ds(start, HD), :], k_gain, table, BF16)
    turned_ref[...] = v_ref[...].astype(F32).T
    kvt_ref[HD:, :] = turned_ref[pl.ds(start, HD), :].astype(BF16)


def prep(place, queries, key_input, value_input, q_gain, k_gain, table, heads):
    rows = queries.shape[0]
    return call(
        functools.partial(prep_body, heads=heads, group=HEADS // KV_HEADS),
        place,
        (queries, key_input, value_input, q_gain, k_gain, table),
        [
            full(queries.shape),
            full(key_input.shape),
            full(value_input.shape),
            full(q_gain.shape),
            full(k_gain.shape),
            pl.BlockSpec((table.shape[0], rows), lambda i, place: (0, place[1])),
        ],
        [
            jax.ShapeDtypeStruct((queries.shape[1], rows), BF16),
            jax.ShapeDtypeStruct((2 * HD, rows), BF16),
        ],
        scratch=[pltpu.VMEM((key_input.shape[1], rows), F32)],
        micros=1.5,
    )


def attend_body(place, qt_ref, *refs, blocks, heads, groups):
    count = len(refs) - 5 - groups
    kv_refs, out_refs = refs[:count], refs[count : count + groups]
    out_ref, k_ref, v_ref, num_ref, den_ref = refs[count + groups :]
    keys = kv_refs[0].shape[1]
    per = blocks // count
    for b in range(blocks):
        base = (b % per) * 2 * HD
        k_ref[b] = kv_refs[b // per][base : base + HD, :].astype(F32).T.astype(BF16)
        v_ref[b] = kv_refs[b // per][base + HD : base + 2 * HD, :]
    num_ref[...] = jnp.zeros_like(num_ref)
    den_ref[...] = jnp.zeros_like(den_ref)

    def one(b, carry):
        k = k_ref[b]
        v = v_ref[b]
        for h in range(heads):
            q = qt_ref[h * HD : (h + 1) * HD, :]
            p = jnp.exp2(mm(k, q) * (LOG2E * HD**-0.5))
            den_ref[h * 8 : (h + 1) * 8, :] += jnp.sum(p.reshape(keys // 8, 8, p.shape[1]), axis=0)
            num_ref[h * HD : (h + 1) * HD, :] += mm(v, p.astype(BF16))
        return carry

    lax.fori_loop(0, blocks, one, 0)
    for h in range(heads):
        den = jnp.sum(den_ref[h * 8 : (h + 1) * 8, :], axis=0, keepdims=True)
        num_ref[h * HD : (h + 1) * HD, :] = num_ref[h * HD : (h + 1) * HD, :] / den
    out_ref[...] = num_ref[...].T
    rows = out_refs[0].shape[0]
    for k in range(groups):
        at = pl.multiple_of((place[0] ^ k) * rows, rows)
        out_refs[k][...] = out_ref[pl.ds(at, rows), :].astype(BF16)


def attend(place, qt, kv_blocks, heads, groups):
    rows = qt.shape[1]
    keys = kv_blocks[0].shape[1]
    blocks = sum(b.shape[0] for b in kv_blocks) // (2 * HD)
    return call(
        functools.partial(attend_body, blocks=blocks, heads=heads, groups=groups),
        place,
        (qt, *kv_blocks),
        [full(qt.shape)] + [full(b.shape) for b in kv_blocks],
        [jax.ShapeDtypeStruct((rows // groups, qt.shape[0]), BF16)] * groups,
        scratch=[
            pltpu.VMEM((rows, qt.shape[0]), F32),
            pltpu.VMEM((blocks, keys, HD), BF16),
            pltpu.VMEM((blocks, HD, keys), BF16),
            pltpu.VMEM(qt.shape, F32),
            pltpu.VMEM((heads * 8, rows), F32),
        ],
        micros=12.0,
    )


def mix_body(place, *refs, groups):
    att_refs, w_refs, out_ref = refs[:groups], refs[groups : 2 * groups], refs[2 * groups]
    total = jnp.zeros(out_ref.shape, F32)
    for k in range(groups):
        total += mm(att_refs[k][...], w_refs[k][...]).astype(BF16).astype(F32)
    out_ref[...] = total.astype(BF16)


def mix(place, atts, weights):
    groups = len(weights)
    rows = atts[0].shape[0]
    depth, width = weights[0].shape
    tile = min(width, 512)
    return call(
        functools.partial(mix_body, groups=groups),
        place,
        (*atts, *weights),
        [full(a.shape) for a in atts] + [pl.BlockSpec((depth, tile), lambda j, place: (0, j))] * groups,
        [jax.ShapeDtypeStruct((rows, width), BF16)],
        grid=(width // tile,),
        out_specs=[pl.BlockSpec((rows, tile), lambda j, place: (0, j))],
        micros=2.5,
    )[0]


def expert_body(place, *refs, groups, tile):
    x_refs = refs[:groups]
    gain_ref, gate_hbm, up_hbm, down_hbm = refs[groups : groups + 4]
    out_refs = refs[groups + 4 : 2 * groups + 4]
    scaled_ref, hidden_ref, gate_ref, up_ref, down_ref, gate_sem, up_sem, down_sem = refs[2 * groups + 4 :]
    feat = x_refs[0].shape[1]
    width = groups * feat
    steps = gate_ref.shape[0]

    def spot(k):
        return pl.ds(pl.multiple_of((place[0] ^ k) * feat, feat), feat)

    def fetch_gate(j):
        cols = pl.ds(pl.multiple_of(j * tile, tile), tile)
        return pltpu.make_async_copy(gate_hbm.at[0, :, cols], gate_ref.at[j], gate_sem.at[j])

    def fetch_up(j):
        cols = pl.ds(pl.multiple_of(j * tile, tile), tile)
        return pltpu.make_async_copy(up_hbm.at[0, :, cols], up_ref.at[j], up_sem.at[j])

    def fetch_down(k):
        return pltpu.make_async_copy(down_hbm.at[0, :, spot(k)], down_ref.at[k], down_sem.at[k])

    for j in range(steps):
        fetch_gate(j).start()
        fetch_up(j).start()
    for k in range(groups):
        fetch_down(k).start()

    squares = 0.0
    for k in range(groups):
        x = x_refs[k][...].astype(F32)
        scaled_ref[:, spot(k)] = (x * gain_ref[:, spot(k)]).astype(BF16)
        squares += jnp.sum(x * x, axis=1, keepdims=True)
    scale = lax.rsqrt(squares / width + EPSILON)

    def one(j, carry):
        x = scaled_ref[...]
        fetch_gate(j).wait()
        gate = mm(x, gate_ref[j]) * scale
        fetch_up(j).wait()
        up = mm(x, up_ref[j]) * scale
        cols = pl.ds(pl.multiple_of(j * tile, tile), tile)
        hidden_ref[:, cols] = (gate / (1.0 + jnp.exp(-gate)) * up).astype(BF16)
        return carry

    lax.fori_loop(0, steps, one, 0)
    for k in range(groups):
        fetch_down(k).wait()
        out_refs[k][...] = mm(hidden_ref[...], down_ref[k]).astype(BF16)


def expert(place, xs, gain, gate, up, down):
    groups = len(xs)
    rows, feat = xs[0].shape
    depth, ff = gate.shape[1:]
    tile = min(ff, 256)
    steps = ff // tile
    return call(
        functools.partial(expert_body, groups=groups, tile=tile),
        place,
        (*xs, gain, gate, up, down),
        [full(x.shape) for x in xs] + [full(gain.shape), hbm(), hbm(), hbm()],
        [jax.ShapeDtypeStruct((rows, feat), BF16)] * groups,
        scratch=[
            pltpu.VMEM((rows, depth), BF16),
            pltpu.VMEM((rows, ff), BF16),
            pltpu.VMEM((steps, depth, tile), BF16),
            pltpu.VMEM((steps, depth, tile), BF16),
            pltpu.VMEM((groups, ff, feat), BF16),
            pltpu.SemaphoreType.DMA((steps,)),
            pltpu.SemaphoreType.DMA((steps,)),
            pltpu.SemaphoreType.DMA((groups,)),
        ],
        micros=9.0,
    )


def combine_body(place, slot_ref, scores_ref, *refs, chunks):
    row_refs, out_ref = refs[:chunks], refs[chunks]
    tokens = out_ref.shape[0]
    slots = row_refs[0].shape[0]
    scores = scores_ref[...]
    weight = scores / jnp.sum(scores, axis=0, keepdims=True)
    slot = slot_ref[...]
    total = jnp.zeros(out_ref.shape, F32)
    for k in range(2):
        picked = jnp.zeros(out_ref.shape, F32)
        for c in range(chunks):
            rows = lax.broadcasted_iota(jnp.int32, (slots, tokens), 0) + c * slots
            pick = (rows == slot[k : k + 1, :]).astype(F32).astype(BF16)
            picked += mm(pick, row_refs[c][...], ((0,), (0,)))
        total += picked * column(weight[k : k + 1, :])
    out_ref[...] = total.astype(BF16)


def combine(place, slot, scores, rows):
    return call(
        functools.partial(combine_body, chunks=len(rows)),
        place,
        (slot, scores, *rows),
        [full(slot.shape), full(scores.shape)] + [full(r.shape) for r in rows],
        [jax.ShapeDtypeStruct((slot.shape[1], rows[0].shape[1]), BF16)],
        micros=1.5,
    )[0]


def local(
    table,
    queries,
    key_input,
    value_input,
    query_gain,
    key_gain,
    mix_out_weight,
    expert_input,
    ffn_gain,
    routes,
    route_scores,
    gate_weight,
    up_weight,
    down_weight,
):
    n_ep = lax.axis_size("ep")
    n_tp = lax.axis_size("tp")
    heads = queries.shape[1] // HD
    tokens, top = routes.shape
    width = expert_input.shape[1]
    feat = width // n_tp
    cap = 3 * tokens * top // (2 * n_ep)
    unit = 8 * CHUNKS
    cap = -(-cap // unit) * unit
    place = jnp.stack([lax.axis_index("tp"), lax.axis_index("ep")]).astype(jnp.int32)

    weights = {0: mix_out_weight}
    for k in range(2, n_tp, 2):
        weights[k] = send(mix_out_weight, "tp", k)

    *outbound, slot = dispatch(place, routes.T, expert_input, n_ep, cap, CHUNKS, feat)
    arrived = [lax.all_to_all(o, "ep", split_axis=0, concat_axis=0, tiled=True) for o in outbound]

    qt, kvt = prep(
        place, queries, key_input, value_input, query_gain[None], key_gain[None], table, heads
    )
    pair = jnp.concatenate([kvt, send(kvt, "ep", 1)], axis=0)
    blocks = [pair] + [send(pair, "ep", k) for k in sorted(range(2, n_ep, 2), key=lambda k: k ^ (n_ep // 2))]

    reduced = []
    for a in arrived:
        xs = {0: a}
        for k in range(2, n_tp, 2):
            xs[k] = send(a, "tp", k)
        for k in range(0, n_tp, 2):
            xs[k + 1] = send(xs[k], "tp", 1)
        parts = expert(
            place, [xs[k] for k in range(n_tp)], ffn_gain[None], gate_weight, up_weight, down_weight
        )
        other = {k: send(parts[k + 1], "tp", 1) for k in range(0, n_tp, 2)}
        total = parts[0].astype(F32) + other[0].astype(F32)
        for k in range(2, n_tp, 2):
            both = (parts[k].astype(F32) + other[k].astype(F32)).astype(BF16)
            total += send(both, "tp", k).astype(F32)
        reduced.append(total.astype(BF16))

    for k in range(0, n_tp, 2):
        weights[k + 1] = send(weights[k], "tp", 1)
    atts = attend(place, qt, blocks, heads, n_tp)
    atts = [atts[0]] + [send(atts[k], "tp", k) for k in range(1, n_tp)]
    mixed = mix(place, atts, [weights[k] for k in range(n_tp)])

    returned = [lax.all_to_all(r, "ep", split_axis=0, concat_axis=0, tiled=True) for r in reduced]
    out = combine(place, slot, route_scores.T, returned)
    return mixed, out


def solution(mesh):
    n_ep = mesh.shape["ep"]
    placed = (
        P(),
        P("ep", "tp"),
        P("ep", None),
        P("ep", None),
        P(),
        P(),
        P("tp", None),
        P("ep", None),
        P(),
        P("ep", None),
        P("ep", None),
        P("ep", None, "tp"),
        P("ep", None, "tp"),
        P("ep", "tp", None),
    )

    step = jax.shard_map(
        local,
        mesh=mesh,
        in_specs=placed,
        out_specs=(P(("ep", "tp"), None), P("ep", "tp")),
        check_vma=False,
    )

    def run(queries, *rest):
        table = jnp.asarray(rope_tables(queries.shape[0] // n_ep, n_ep))
        return step(table, queries, *rest)

    return run
```

```python
import functools

import jax
import jax.numpy as jnp
import numpy as np
from jax import lax
from jax.experimental import pallas as pl
from jax.experimental.pallas import tpu as pltpu
from jax.sharding import PartitionSpec as P


HEADS = 16
KV_HEADS = 4
HD = 64
GRID_W = 64
EPSILON = 1e-06
ROPE_BASE = 10000.0
LOG2E = 1.4426950408889634
F32 = jnp.float32
BF16 = jnp.bfloat16
VMEM_LIMIT = 48 * 1024 * 1024
FLOPS_PER_MICRO = 500_000_000


def full(shape):
    return pl.BlockSpec(shape, lambda *_: (0,) * len(shape))


def hbm():
    return pl.BlockSpec(memory_space=pltpu.HBM)


def call(body, place, args, in_specs, outs, grid=(1,), scratch=(), out_specs=None, micros=1.0):
    return pl.pallas_call(
        body,
        grid_spec=pltpu.PrefetchScalarGridSpec(
            num_scalar_prefetch=1,
            grid=grid,
            in_specs=in_specs,
            out_specs=[full(o.shape) for o in outs] if out_specs is None else out_specs,
            scratch_shapes=list(scratch),
        ),
        out_shape=outs,
        cost_estimate=pl.CostEstimate(
            flops=int(micros * FLOPS_PER_MICRO), transcendentals=0, bytes_accessed=0
        ),
        compiler_params=pltpu.CompilerParams(
            dimension_semantics=("arbitrary",) * len(grid), vmem_limit_bytes=VMEM_LIMIT
        ),
    )(place, *args)


def mm(a, b, dims=((1,), (0,))):
    return lax.dot_general(a, b, (dims, ((), ())), preferred_element_type=F32)


def send(x, axis, flip):
    n = lax.axis_size(axis)
    return lax.ppermute(x, axis, [(i, i ^ flip) for i in range(n)])


def dispatch_body(place, routes_ref, x_hbm, *outs, experts, cap):
    out_ref, slot_ref, x_ref, sem = outs
    tokens, feat = x_ref.shape
    cols = pl.ds(pl.multiple_of(place[0] * feat, feat), feat)
    fetch = pltpu.make_async_copy(x_hbm.at[:, cols], x_ref, sem)
    fetch.start()
    routes = routes_ref[...]
    rows = lax.broadcasted_iota(jnp.int32, (experts, tokens), 0)
    first = (rows == routes[0:1, :]).astype(F32)
    second = (rows == routes[1:2, :]).astype(F32)
    hits = first + second
    row = lax.broadcasted_iota(jnp.int32, (tokens, tokens), 0)
    col = lax.broadcasted_iota(jnp.int32, (tokens, tokens), 1)
    before = (row < col).astype(F32).astype(BF16)
    count = mm(hits.astype(BF16), before)
    slot = jnp.where(hits > 0.5, count, -1.0).astype(jnp.int32)

    def flat(choice, expert):
        at = jnp.sum(count * choice, axis=0, keepdims=True).astype(jnp.int32)
        return (expert ^ place[1] ^ (experts // 2)) * cap + at

    slot_ref[0:1, :] = flat(first, routes[0:1, :])
    slot_ref[1:2, :] = flat(second, routes[1:2, :])
    fetch.wait()
    x = x_ref[...]
    slots = lax.broadcasted_iota(jnp.int32, (cap, tokens), 0)
    for e in range(experts):
        pick = (slots == slot[e : e + 1, :]).astype(F32).astype(BF16)
        out_ref[e * cap : (e + 1) * cap, :] = mm(pick, x).astype(BF16)


def dispatch(place, routes, expert_input, experts, cap, feat):
    tokens = routes.shape[1]
    outs = [jax.ShapeDtypeStruct((experts * cap, feat), BF16), jax.ShapeDtypeStruct((2, tokens), jnp.int32)]
    return call(
        functools.partial(dispatch_body, experts=experts, cap=cap),
        place,
        (routes, expert_input),
        [full(routes.shape), hbm()],
        outs,
        scratch=[pltpu.VMEM((tokens, feat), BF16), pltpu.SemaphoreType.DMA],
        micros=1.5,
    )


def rope_tables(token_count, n_ep):
    quarter = HD // 4
    inverse = (np.float32(ROPE_BASE) ** (-np.arange(quarter, dtype=np.float32) / np.float32(quarter))).astype(
        np.float32
    )
    pos = np.arange(token_count * n_ep)

    def both(steps):
        angle = (inverse[:, None] * steps.astype(np.float32)[None, :]).astype(np.float32).astype(np.float64)
        return np.concatenate([np.cos(angle), np.sin(angle)], 0).astype(np.float32)

    return np.concatenate([both(pos // GRID_W), both(pos % GRID_W)], 0)


def turn(x, gain, table, low):
    quarter = HD // 4
    x = x.astype(F32)
    scale = lax.rsqrt(jnp.mean(x * x, axis=0, keepdims=True) + EPSILON)
    x = x * scale * gain
    u0, w0, u1, w1 = (x[i * quarter : (i + 1) * quarter] for i in range(4))
    cr, sr, cc, sc = (table[i * quarter : (i + 1) * quarter] for i in range(4))
    return jnp.concatenate(
        [u0 * cr - w0 * sr, w0 * cr + u0 * sr, u1 * cc - w1 * sc, w1 * cc + u1 * sc], axis=0
    ).astype(low)


def column(row):
    n = row.shape[1]
    same = lax.broadcasted_iota(jnp.int32, (n, n), 0) == lax.broadcasted_iota(jnp.int32, (n, n), 1)
    return jnp.sum(jnp.where(same, row, 0.0), axis=1, keepdims=True)


def prep_body(
    place,
    q_hbm,
    k_hbm,
    v_hbm,
    q_gain_ref,
    k_gain_ref,
    table_hbm,
    qt_ref,
    kvt_ref,
    turned_ref,
    q_ref,
    k_ref,
    v_ref,
    table_ref,
    sems,
    *,
    heads,
    group,
):
    rows = q_ref.shape[0]
    cols = pl.ds(pl.multiple_of(place[1] * rows, rows), rows)
    copies = [
        pltpu.make_async_copy(src, dst, sems.at[i])
        for i, (src, dst) in enumerate(
            ((k_hbm, k_ref), (table_hbm.at[:, cols], table_ref), (v_hbm, v_ref), (q_hbm, q_ref))
        )
    ]
    for c in copies:
        c.start()
    for c in copies:
        c.wait()
    table = table_ref[...]
    q_gain = column(q_gain_ref[...])
    k_gain = column(k_gain_ref[...])
    qt = q_ref[...].astype(F32).T
    for h in range(heads):
        qt_ref[h * HD : (h + 1) * HD, :] = turn(qt[h * HD : (h + 1) * HD], q_gain, table, BF16)
    start = pl.multiple_of((place[0] * heads // group) * HD, HD)
    turned_ref[...] = k_ref[...].astype(F32).T
    kvt_ref[:HD, :] = turn(turned_ref[pl.ds(start, HD), :], k_gain, table, BF16)
    turned_ref[...] = v_ref[...].astype(F32).T
    kvt_ref[HD:, :] = turned_ref[pl.ds(start, HD), :].astype(BF16)


def prep(place, queries, key_input, value_input, q_gain, k_gain, table, heads):
    rows = queries.shape[0]
    return call(
        functools.partial(prep_body, heads=heads, group=HEADS // KV_HEADS),
        place,
        (queries, key_input, value_input, q_gain, k_gain, table),
        [
            hbm(),
            hbm(),
            hbm(),
            full(q_gain.shape),
            full(k_gain.shape),
            hbm(),
        ],
        [
            jax.ShapeDtypeStruct((queries.shape[1], rows), BF16),
            jax.ShapeDtypeStruct((2 * HD, rows), BF16),
        ],
        scratch=[
            pltpu.VMEM((key_input.shape[1], rows), F32),
            pltpu.VMEM(queries.shape, BF16),
            pltpu.VMEM(key_input.shape, BF16),
            pltpu.VMEM(value_input.shape, BF16),
            pltpu.VMEM((table.shape[0], rows), F32),
            pltpu.SemaphoreType.DMA((4,)),
        ],
        micros=2.0,
    )


def attend_body(place, qt_ref, *refs, blocks, heads, groups):
    count = len(refs) - 5 - groups
    kv_refs, out_refs = refs[:count], refs[count : count + groups]
    out_ref, k_ref, v_ref, num_ref, den_ref = refs[count + groups :]
    keys = kv_refs[0].shape[1]
    per = blocks // count
    for b in range(blocks):
        base = (b % per) * 2 * HD
        k_ref[b] = kv_refs[b // per][base : base + HD, :].astype(F32).T.astype(BF16)
        v_ref[b] = kv_refs[b // per][base + HD : base + 2 * HD, :]
    num_ref[...] = jnp.zeros_like(num_ref)
    den_ref[...] = jnp.zeros_like(den_ref)

    def one(b, carry):
        k = k_ref[b]
        v = v_ref[b]
        for h in range(heads):
            q = qt_ref[h * HD : (h + 1) * HD, :]
            p = jnp.exp2(mm(k, q) * (LOG2E * HD**-0.5))
            den_ref[h * 8 : (h + 1) * 8, :] += jnp.sum(p.reshape(keys // 8, 8, p.shape[1]), axis=0)
            num_ref[h * HD : (h + 1) * HD, :] += mm(v, p.astype(BF16))
        return carry

    lax.fori_loop(0, blocks, one, 0)
    for h in range(heads):
        den = jnp.sum(den_ref[h * 8 : (h + 1) * 8, :], axis=0, keepdims=True)
        num_ref[h * HD : (h + 1) * HD, :] = num_ref[h * HD : (h + 1) * HD, :] / den
    out_ref[...] = num_ref[...].T
    rows = out_refs[0].shape[0]
    for k in range(groups):
        at = pl.multiple_of((place[0] ^ k) * rows, rows)
        out_refs[k][...] = out_ref[pl.ds(at, rows), :].astype(BF16)


def attend(place, qt, kv_blocks, heads, groups):
    rows = qt.shape[1]
    keys = kv_blocks[0].shape[1]
    blocks = sum(b.shape[0] for b in kv_blocks) // (2 * HD)
    return call(
        functools.partial(attend_body, blocks=blocks, heads=heads, groups=groups),
        place,
        (qt, *kv_blocks),
        [full(qt.shape)] + [full(b.shape) for b in kv_blocks],
        [jax.ShapeDtypeStruct((rows // groups, qt.shape[0]), BF16)] * groups,
        scratch=[
            pltpu.VMEM((rows, qt.shape[0]), F32),
            pltpu.VMEM((blocks, keys, HD), BF16),
            pltpu.VMEM((blocks, HD, keys), BF16),
            pltpu.VMEM(qt.shape, F32),
            pltpu.VMEM((heads * 8, rows), F32),
        ],
        micros=12.0,
    )


def mix_body(place, *refs, groups):
    att_refs, w_refs, out_ref = refs[:groups], refs[groups : 2 * groups], refs[2 * groups]
    total = jnp.zeros(out_ref.shape, F32)
    for k in range(groups):
        total += mm(att_refs[k][...], w_refs[k][...]).astype(BF16).astype(F32)
    out_ref[...] = total.astype(BF16)


def mix(place, atts, weights):
    groups = len(weights)
    rows = atts[0].shape[0]
    depth, width = weights[0].shape
    tile = min(width, 512)
    return call(
        functools.partial(mix_body, groups=groups),
        place,
        (*atts, *weights),
        [full(a.shape) for a in atts] + [pl.BlockSpec((depth, tile), lambda j, place: (0, j))] * groups,
        [jax.ShapeDtypeStruct((rows, width), BF16)],
        grid=(width // tile,),
        out_specs=[pl.BlockSpec((rows, tile), lambda j, place: (0, j))],
        micros=2.5,
    )[0]


def expert_body(place, *refs, groups, tile, experts):
    x_refs = refs[:groups]
    gain_ref, gate_hbm, up_hbm, down_hbm = refs[groups : groups + 4]
    out_refs = refs[groups + 4 : 3 * groups + 4]
    scaled_ref, hidden_ref, gate_ref, up_ref, down_ref, gate_sem, up_sem, down_sem = refs[3 * groups + 4 :]
    rows, feat = x_refs[0].shape
    cap = rows // experts
    half = rows // 2
    width = groups * feat
    steps = gate_ref.shape[0]

    def spot(k):
        return pl.ds(pl.multiple_of((place[0] ^ k) * feat, feat), feat)

    def fetch_gate(j):
        cols = slice(j * tile, (j + 1) * tile)
        return pltpu.make_async_copy(gate_hbm.at[0, :, cols], gate_ref.at[j], gate_sem.at[j])

    def fetch_up(j):
        cols = slice(j * tile, (j + 1) * tile)
        return pltpu.make_async_copy(up_hbm.at[0, :, cols], up_ref.at[j], up_sem.at[j])

    def fetch_down(k):
        return pltpu.make_async_copy(down_hbm.at[0, :, spot(k)], down_ref.at[k], down_sem.at[k])

    fetch_gate(0).start()
    fetch_up(0).start()
    parts = []
    for i in range(experts):
        at = pl.multiple_of((place[1] ^ i ^ (experts // 2)) * cap, cap)
        squares = 0.0
        for k in range(groups):
            x = x_refs[k][pl.ds(at, cap), :].astype(F32)
            scaled_ref[i * cap : (i + 1) * cap, spot(k)] = (x * gain_ref[:, spot(k)]).astype(BF16)
            squares += x * x
        parts.append(jnp.sum(squares, axis=1, keepdims=True))
    scale = lax.rsqrt(jnp.concatenate(parts, axis=0) / width + EPSILON)

    waiting = list(range(groups))
    share = -(-groups // steps)
    started = []
    for j in range(steps):
        if j + 1 < steps:
            fetch_gate(j + 1).start()
            fetch_up(j + 1).start()
        for k in waiting[:share]:
            fetch_down(k).start()
            started.append(k)
        waiting = waiting[share:]
        x = scaled_ref[...]
        fetch_gate(j).wait()
        gate = mm(x, gate_ref[j]) * scale
        fetch_up(j).wait()
        up = mm(x, up_ref[j]) * scale
        hidden_ref[:, j * tile : (j + 1) * tile] = (gate / (1.0 + jnp.exp(-gate)) * up).astype(BF16)
    for k in range(groups):
        fetch_down(k).wait()
        part = mm(hidden_ref[...], down_ref[k]).astype(BF16)
        out_refs[2 * k][...] = part[:half]
        out_refs[2 * k + 1][...] = part[half:]


def expert(place, xs, gain, gate, up, down, experts):
    groups = len(xs)
    rows, feat = xs[0].shape
    depth, ff = gate.shape[1:]
    tile = min(ff, 256)
    steps = ff // tile
    return call(
        functools.partial(expert_body, groups=groups, tile=tile, experts=experts),
        place,
        (*xs, gain, gate, up, down),
        [full(x.shape) for x in xs] + [full(gain.shape), hbm(), hbm(), hbm()],
        [jax.ShapeDtypeStruct((rows // 2, feat), BF16)] * (2 * groups),
        scratch=[
            pltpu.VMEM((rows, depth), BF16),
            pltpu.VMEM((rows, ff), BF16),
            pltpu.VMEM((steps, depth, tile), BF16),
            pltpu.VMEM((steps, depth, tile), BF16),
            pltpu.VMEM((groups, ff, feat), BF16),
            pltpu.SemaphoreType.DMA((steps,)),
            pltpu.SemaphoreType.DMA((steps,)),
            pltpu.SemaphoreType.DMA((groups,)),
        ],
        micros=11.0,
    )


def finish_body(place, *refs, terms):
    total = 0.0
    for r in refs[:terms]:
        total += r[...].astype(F32)
    total = total.astype(BF16)
    outs = refs[terms:]
    rows = outs[0].shape[0]
    for i, o in enumerate(outs):
        o[...] = total[i * rows : (i + 1) * rows]


def finish(place, terms, pieces):
    rows, feat = terms[0].shape
    return call(
        functools.partial(finish_body, terms=len(terms)),
        place,
        tuple(terms),
        [full(t.shape) for t in terms],
        [jax.ShapeDtypeStruct((rows // pieces, feat), BF16)] * pieces,
        micros=0.5,
    )


def combine_body(place, slot_ref, scores_ref, *refs, blocks):
    out_ref, rows_ref = refs[blocks:]
    tokens = out_ref.shape[0]
    cap = refs[0].shape[0]
    for i in range(blocks):
        rows_ref[i * cap : (i + 1) * cap, :] = refs[i][...]
    scores = scores_ref[...]
    weight = scores / jnp.sum(scores, axis=0, keepdims=True)
    slot = slot_ref[...]
    rows = lax.broadcasted_iota(jnp.int32, (blocks * cap, tokens), 0)
    total = jnp.zeros(out_ref.shape, F32)
    for k in range(2):
        pick = (rows == slot[k : k + 1, :]).astype(F32).astype(BF16)
        total += mm(pick, rows_ref[...], ((0,), (0,))) * column(weight[k : k + 1, :])
    out_ref[...] = total.astype(BF16)


def combine(place, slot, scores, rows):
    cap, feat = rows[0].shape
    return call(
        functools.partial(combine_body, blocks=len(rows)),
        place,
        (slot, scores, *rows),
        [full(slot.shape), full(scores.shape)] + [full(r.shape) for r in rows],
        [jax.ShapeDtypeStruct((slot.shape[1], feat), BF16)],
        scratch=[pltpu.VMEM((len(rows) * cap, feat), BF16)],
        micros=1.5,
    )[0]


def local(
    table,
    queries,
    key_input,
    value_input,
    query_gain,
    key_gain,
    mix_out_weight,
    expert_input,
    ffn_gain,
    routes,
    route_scores,
    gate_weight,
    up_weight,
    down_weight,
):
    n_ep = lax.axis_size("ep")
    n_tp = lax.axis_size("tp")
    heads = queries.shape[1] // HD
    tokens, top = routes.shape
    width = expert_input.shape[1]
    feat = width // n_tp
    cap = 3 * tokens * top // (2 * n_ep)
    cap = -(-cap // 8) * 8
    place = jnp.stack([lax.axis_index("tp"), lax.axis_index("ep")]).astype(jnp.int32)
    half = n_ep // 2

    weights = {0: mix_out_weight}
    for k in range(2, n_tp, 2):
        weights[k] = send(mix_out_weight, "tp", k)
    for k in range(0, n_tp, 2):
        weights[k + 1] = send(weights[k], "tp", 1)

    qt, kvt = prep(
        place, queries, key_input, value_input, query_gain[None], key_gain[None], table, heads
    )
    blocks = [kvt]
    blocks += [send(kvt, "ep", k) for k in range(n_ep - 2, 0, -2)]
    blocks.append(send(kvt, "ep", 1))
    blocks += [send(b, "ep", 1) for b in blocks[1:half]]

    outbound, slot = dispatch(place, routes.T, expert_input, n_ep, cap, feat)
    arrived = lax.all_to_all(outbound, "ep", split_axis=0, concat_axis=0, tiled=True)
    xs = {0: arrived}
    for k in range(2, n_tp, 2):
        xs[k] = send(arrived, "tp", k)
    for k in range(0, n_tp, 2):
        xs[k + 1] = send(xs[k], "tp", 1)

    atts = attend(place, qt, blocks, heads, n_tp)
    atts = [atts[0]] + [send(atts[k], "tp", k) for k in range(1, n_tp)]

    parts = expert(
        place, [xs[k] for k in range(n_tp)], ffn_gain[None], gate_weight, up_weight, down_weight, n_ep
    )
    returned = []
    for side in range(2):
        mine = {k: (parts[2 * k + side], send(parts[2 * k + 2 + side], "tp", 1)) for k in range(0, n_tp, 2)}
        terms = list(mine[0])
        for k in range(2, n_tp, 2):
            (both,) = finish(place, mine[k], 1)
            terms.append(send(both, "tp", k))
        pieces = finish(place, terms, half)
        for i, piece in enumerate(pieces):
            k = i ^ half if side == 0 else i
            returned.append(send(piece, "ep", k) if k else piece)

    mixed = mix(place, atts, [weights[k] for k in range(n_tp)])
    out = combine(place, slot, route_scores.T, returned)
    return mixed, out


def solution(mesh):
    n_ep = mesh.shape["ep"]
    placed = (
        P(),
        P("ep", "tp"),
        P("ep", None),
        P("ep", None),
        P(),
        P(),
        P("tp", None),
        P("ep", None),
        P(),
        P("ep", None),
        P("ep", None),
        P("ep", None, "tp"),
        P("ep", None, "tp"),
        P("ep", "tp", None),
    )

    step = jax.shard_map(
        local,
        mesh=mesh,
        in_specs=placed,
        out_specs=(P(("ep", "tp"), None), P("ep", "tp")),
        check_vma=False,
    )

    def run(queries, *rest):
        table = jnp.asarray(rope_tables(queries.shape[0] // n_ep, n_ep))
        return step(table, queries, *rest)

    return run
```

```python
import functools

import jax
import jax.numpy as jnp
import numpy as np
from jax import lax
from jax.experimental import pallas as pl
from jax.experimental.pallas import tpu as pltpu
from jax.sharding import PartitionSpec as P


HEADS = 16
KV_HEADS = 4
HD = 64
GRID_W = 64
EPSILON = 1e-06
ROPE_BASE = 10000.0
LOG2E = 1.4426950408889634
F32 = jnp.float32
BF16 = jnp.bfloat16
VMEM_LIMIT = 24 * 1024 * 1024
FLOPS_PER_MICRO = 500_000_000


def full(shape):
    return pl.BlockSpec(shape, lambda *_: (0,) * len(shape))


def hbm():
    return pl.BlockSpec(memory_space=pltpu.HBM)


def far_memory(x):
    return pltpu.with_memory_space_constraint(x, pltpu.HBM)


def call(body, place, args, in_specs, outs, grid=(1,), scratch=(), out_specs=None, micros=1.0):
    return pl.pallas_call(
        body,
        grid_spec=pltpu.PrefetchScalarGridSpec(
            num_scalar_prefetch=1,
            grid=grid,
            in_specs=in_specs,
            out_specs=[full(o.shape) for o in outs] if out_specs is None else out_specs,
            scratch_shapes=list(scratch),
        ),
        out_shape=outs,
        cost_estimate=pl.CostEstimate(
            flops=int(micros * FLOPS_PER_MICRO), transcendentals=0, bytes_accessed=0
        ),
        compiler_params=pltpu.CompilerParams(
            dimension_semantics=("arbitrary",) * len(grid), vmem_limit_bytes=VMEM_LIMIT
        ),
    )(place, *args)


def mm(a, b, dims=((1,), (0,))):
    return lax.dot_general(a, b, (dims, ((), ())), preferred_element_type=F32)


def send(x, axis, flip):
    n = lax.axis_size(axis)
    return lax.ppermute(x, axis, [(i, i ^ flip) for i in range(n)])


def dispatch_body(place, routes_ref, x_hbm, *outs, experts, cap):
    out_ref, slot_ref, x_ref, sem = outs
    tokens, feat = x_ref.shape
    cols = pl.ds(pl.multiple_of(place[0] * feat, feat), feat)
    fetch = pltpu.make_async_copy(x_hbm.at[:, cols], x_ref, sem)
    fetch.start()
    routes = routes_ref[...]
    rows = lax.broadcasted_iota(jnp.int32, (experts, tokens), 0)
    first = (rows == routes[0:1, :]).astype(F32)
    second = (rows == routes[1:2, :]).astype(F32)
    hits = first + second
    row = lax.broadcasted_iota(jnp.int32, (tokens, tokens), 0)
    col = lax.broadcasted_iota(jnp.int32, (tokens, tokens), 1)
    before = (row < col).astype(F32).astype(BF16)
    count = mm(hits.astype(BF16), before)
    slot = jnp.where(hits > 0.5, count, -1.0).astype(jnp.int32)

    def flat(choice, expert):
        at = jnp.sum(count * choice, axis=0, keepdims=True).astype(jnp.int32)
        return (expert ^ place[1] ^ (experts // 2)) * cap + at

    slot_ref[0:1, :] = flat(first, routes[0:1, :])
    slot_ref[1:2, :] = flat(second, routes[1:2, :])
    fetch.wait()
    x = x_ref[...]
    slots = lax.broadcasted_iota(jnp.int32, (cap, tokens), 0)
    for e in range(experts):
        pick = (slots == slot[e : e + 1, :]).astype(F32).astype(BF16)
        out_ref[e * cap : (e + 1) * cap, :] = mm(pick, x).astype(BF16)


def dispatch(place, routes, expert_input, experts, cap, feat):
    tokens = routes.shape[1]
    outs = [jax.ShapeDtypeStruct((experts * cap, feat), BF16), jax.ShapeDtypeStruct((2, tokens), jnp.int32)]
    return call(
        functools.partial(dispatch_body, experts=experts, cap=cap),
        place,
        (routes, expert_input),
        [full(routes.shape), hbm()],
        outs,
        scratch=[pltpu.VMEM((tokens, feat), BF16), pltpu.SemaphoreType.DMA],
        micros=1.5,
    )


def rope_tables(token_count, n_ep):
    quarter = HD // 4
    inverse = (np.float32(ROPE_BASE) ** (-np.arange(quarter, dtype=np.float32) / np.float32(quarter))).astype(
        np.float32
    )
    pos = np.arange(token_count * n_ep)

    def both(steps):
        angle = (inverse[:, None] * steps.astype(np.float32)[None, :]).astype(np.float32).astype(np.float64)
        return np.concatenate([np.cos(angle), np.sin(angle)], 0).astype(np.float32)

    return np.concatenate([both(pos // GRID_W), both(pos % GRID_W)], 0)


def turn(x, gain, table, low):
    quarter = HD // 4
    x = x.astype(F32)
    scale = lax.rsqrt(jnp.mean(x * x, axis=0, keepdims=True) + EPSILON)
    x = x * scale * gain
    u0, w0, u1, w1 = (x[i * quarter : (i + 1) * quarter] for i in range(4))
    cr, sr, cc, sc = (table[i * quarter : (i + 1) * quarter] for i in range(4))
    return jnp.concatenate(
        [u0 * cr - w0 * sr, w0 * cr + u0 * sr, u1 * cc - w1 * sc, w1 * cc + u1 * sc], axis=0
    ).astype(low)


def column(row):
    n = row.shape[1]
    same = lax.broadcasted_iota(jnp.int32, (n, n), 0) == lax.broadcasted_iota(jnp.int32, (n, n), 1)
    return jnp.sum(jnp.where(same, row, 0.0), axis=1, keepdims=True)


def prep_body(
    place,
    q_hbm,
    k_hbm,
    v_hbm,
    q_gain_ref,
    k_gain_ref,
    table_hbm,
    qt_ref,
    kvt_ref,
    turned_ref,
    q_ref,
    k_ref,
    v_ref,
    table_ref,
    sems,
    *,
    heads,
    group,
):
    rows = q_ref.shape[0]
    cols = pl.ds(pl.multiple_of(place[1] * rows, rows), rows)
    copies = [
        pltpu.make_async_copy(src, dst, sems.at[i])
        for i, (src, dst) in enumerate(
            ((k_hbm, k_ref), (table_hbm.at[:, cols], table_ref), (v_hbm, v_ref), (q_hbm, q_ref))
        )
    ]
    for c in copies:
        c.start()
    for c in copies:
        c.wait()
    table = table_ref[...]
    q_gain = column(q_gain_ref[...])
    k_gain = column(k_gain_ref[...])
    qt = q_ref[...].astype(F32).T
    for h in range(heads):
        qt_ref[h * HD : (h + 1) * HD, :] = turn(qt[h * HD : (h + 1) * HD], q_gain, table, BF16)
    start = pl.multiple_of((place[0] * heads // group) * HD, HD)
    turned_ref[...] = k_ref[...].astype(F32).T
    kvt_ref[:HD, :] = turn(turned_ref[pl.ds(start, HD), :], k_gain, table, BF16)
    turned_ref[...] = v_ref[...].astype(F32).T
    kvt_ref[HD:, :] = turned_ref[pl.ds(start, HD), :].astype(BF16)


def prep(place, queries, key_input, value_input, q_gain, k_gain, table, heads):
    rows = queries.shape[0]
    return call(
        functools.partial(prep_body, heads=heads, group=HEADS // KV_HEADS),
        place,
        (queries, key_input, value_input, q_gain, k_gain, table),
        [
            hbm(),
            hbm(),
            hbm(),
            full(q_gain.shape),
            full(k_gain.shape),
            hbm(),
        ],
        [
            jax.ShapeDtypeStruct((queries.shape[1], rows), BF16),
            jax.ShapeDtypeStruct((2 * HD, rows), BF16),
        ],
        scratch=[
            pltpu.VMEM((key_input.shape[1], rows), F32),
            pltpu.VMEM(queries.shape, BF16),
            pltpu.VMEM(key_input.shape, BF16),
            pltpu.VMEM(value_input.shape, BF16),
            pltpu.VMEM((table.shape[0], rows), F32),
            pltpu.SemaphoreType.DMA((4,)),
        ],
        micros=2.0,
    )


def attend_body(place, qt_ref, *refs, blocks, heads, groups):
    count = len(refs) - 5 - groups
    kv_refs, out_refs = refs[:count], refs[count : count + groups]
    out_ref, k_ref, v_ref, num_ref, den_ref = refs[count + groups :]
    keys = kv_refs[0].shape[1]
    per = blocks // count
    for b in range(blocks):
        base = (b % per) * 2 * HD
        k_ref[b] = kv_refs[b // per][base : base + HD, :].astype(F32).T.astype(BF16)
        v_ref[b] = kv_refs[b // per][base + HD : base + 2 * HD, :]
    num_ref[...] = jnp.zeros_like(num_ref)
    den_ref[...] = jnp.zeros_like(den_ref)

    def one(b, carry):
        k = k_ref[b]
        v = v_ref[b]
        for h in range(heads):
            q = qt_ref[h * HD : (h + 1) * HD, :]
            p = jnp.exp2(mm(k, q) * (LOG2E * HD**-0.5))
            den_ref[h * 8 : (h + 1) * 8, :] += jnp.sum(p.reshape(keys // 8, 8, p.shape[1]), axis=0)
            num_ref[h * HD : (h + 1) * HD, :] += mm(v, p.astype(BF16))
        return carry

    lax.fori_loop(0, blocks, one, 0)
    for h in range(heads):
        den = jnp.sum(den_ref[h * 8 : (h + 1) * 8, :], axis=0, keepdims=True)
        num_ref[h * HD : (h + 1) * HD, :] = num_ref[h * HD : (h + 1) * HD, :] / den
    out_ref[...] = num_ref[...].T
    rows = out_refs[0].shape[0]
    for k in range(groups):
        at = pl.multiple_of((place[0] ^ k) * rows, rows)
        out_refs[k][...] = out_ref[pl.ds(at, rows), :].astype(BF16)


def attend(place, qt, kv_blocks, heads, groups):
    rows = qt.shape[1]
    keys = kv_blocks[0].shape[1]
    blocks = sum(b.shape[0] for b in kv_blocks) // (2 * HD)
    return call(
        functools.partial(attend_body, blocks=blocks, heads=heads, groups=groups),
        place,
        (qt, *kv_blocks),
        [full(qt.shape)] + [full(b.shape) for b in kv_blocks],
        [jax.ShapeDtypeStruct((rows // groups, qt.shape[0]), BF16)] * groups,
        scratch=[
            pltpu.VMEM((rows, qt.shape[0]), F32),
            pltpu.VMEM((blocks, keys, HD), BF16),
            pltpu.VMEM((blocks, HD, keys), BF16),
            pltpu.VMEM(qt.shape, F32),
            pltpu.VMEM((heads * 8, rows), F32),
        ],
        micros=12.0,
    )


def mix_body(place, *refs, groups):
    att_refs, w_refs, out_ref = refs[:groups], refs[groups : 2 * groups], refs[2 * groups]
    total = jnp.zeros(out_ref.shape, F32)
    for k in range(groups):
        total += mm(att_refs[k][...], w_refs[k][...]).astype(BF16).astype(F32)
    out_ref[...] = total.astype(BF16)


def mix(place, atts, weights):
    groups = len(weights)
    rows = atts[0].shape[0]
    depth, width = weights[0].shape
    tile = min(width, 512)
    return call(
        functools.partial(mix_body, groups=groups),
        place,
        (*atts, *weights),
        [full(a.shape) for a in atts] + [pl.BlockSpec((depth, tile), lambda j, place: (0, j))] * groups,
        [jax.ShapeDtypeStruct((rows, width), BF16)],
        grid=(width // tile,),
        out_specs=[pl.BlockSpec((rows, tile), lambda j, place: (0, j))],
        micros=2.5,
    )[0]


def expert_body(place, *refs, groups, tile, experts):
    x_refs = refs[:groups]
    gain_ref, gate_ref, up_ref, down_ref = refs[groups : groups + 4]
    out_refs = refs[groups + 4 : 3 * groups + 4]
    scaled_ref, hidden_ref = refs[3 * groups + 4 :]
    rows, feat = x_refs[0].shape
    cap = rows // experts
    half = rows // 2
    width = groups * feat

    def spot(k):
        return pl.ds(pl.multiple_of((place[0] ^ k) * feat, feat), feat)

    parts = []
    for i in range(experts):
        at = pl.multiple_of((place[1] ^ i ^ (experts // 2)) * cap, cap)
        squares = 0.0
        for k in range(groups):
            x = x_refs[k][pl.ds(at, cap), :].astype(F32)
            scaled_ref[i * cap : (i + 1) * cap, spot(k)] = (x * gain_ref[:, spot(k)]).astype(BF16)
            squares += x * x
        parts.append(jnp.sum(squares, axis=1, keepdims=True))
    scale = lax.rsqrt(jnp.concatenate(parts, axis=0) / width + EPSILON)

    for j in range(gate_ref.shape[1] // tile):
        x = scaled_ref[...]
        cols = slice(j * tile, (j + 1) * tile)
        gate = mm(x, gate_ref[:, cols]) * scale
        up = mm(x, up_ref[:, cols]) * scale
        hidden_ref[:, cols] = (gate / (1.0 + jnp.exp(-gate)) * up).astype(BF16)
    for k in range(groups):
        part = mm(hidden_ref[...], down_ref[:, spot(k)]).astype(BF16)
        out_refs[2 * k][...] = part[:half]
        out_refs[2 * k + 1][...] = part[half:]


def expert(place, xs, gain, gate, up, down, experts):
    groups = len(xs)
    rows, feat = xs[0].shape
    depth, ff = gate.shape
    tile = min(ff, 256)
    vmem = pl.BlockSpec(memory_space=pltpu.VMEM)
    return call(
        functools.partial(expert_body, groups=groups, tile=tile, experts=experts),
        place,
        (*xs, gain, gate, up, down),
        [full(x.shape) for x in xs] + [full(gain.shape), vmem, vmem, vmem],
        [jax.ShapeDtypeStruct((rows // 2, feat), BF16)] * (2 * groups),
        scratch=[pltpu.VMEM((rows, depth), BF16), pltpu.VMEM((rows, ff), BF16)],
        micros=9.0,
    )


def finish_body(place, *refs, terms):
    total = 0.0
    for r in refs[:terms]:
        total += r[...].astype(F32)
    total = total.astype(BF16)
    outs = refs[terms:]
    rows = outs[0].shape[0]
    for i, o in enumerate(outs):
        o[...] = total[i * rows : (i + 1) * rows]


def finish(place, terms, pieces):
    rows, feat = terms[0].shape
    return call(
        functools.partial(finish_body, terms=len(terms)),
        place,
        tuple(terms),
        [full(t.shape) for t in terms],
        [jax.ShapeDtypeStruct((rows // pieces, feat), BF16)] * pieces,
        micros=0.5,
    )


def combine_body(place, slot_ref, scores_ref, *refs, blocks):
    out_ref, rows_ref = refs[blocks:]
    tokens = out_ref.shape[0]
    cap = refs[0].shape[0]
    for i in range(blocks):
        rows_ref[i * cap : (i + 1) * cap, :] = refs[i][...]
    scores = scores_ref[...]
    weight = scores / jnp.sum(scores, axis=0, keepdims=True)
    slot = slot_ref[...]
    rows = lax.broadcasted_iota(jnp.int32, (blocks * cap, tokens), 0)
    total = jnp.zeros(out_ref.shape, F32)
    for k in range(2):
        pick = (rows == slot[k : k + 1, :]).astype(F32).astype(BF16)
        total += mm(pick, rows_ref[...], ((0,), (0,))) * column(weight[k : k + 1, :])
    out_ref[...] = total.astype(BF16)


def combine(place, slot, scores, rows):
    cap, feat = rows[0].shape
    return call(
        functools.partial(combine_body, blocks=len(rows)),
        place,
        (slot, scores, *rows),
        [full(slot.shape), full(scores.shape)] + [full(r.shape) for r in rows],
        [jax.ShapeDtypeStruct((slot.shape[1], feat), BF16)],
        scratch=[pltpu.VMEM((len(rows) * cap, feat), BF16)],
        micros=1.5,
    )[0]


def local(
    table,
    queries,
    key_input,
    value_input,
    query_gain,
    key_gain,
    mix_out_weight,
    expert_input,
    ffn_gain,
    routes,
    route_scores,
    gate_weight,
    up_weight,
    down_weight,
):
    n_ep = lax.axis_size("ep")
    n_tp = lax.axis_size("tp")
    heads = queries.shape[1] // HD
    tokens, top = routes.shape
    width = expert_input.shape[1]
    feat = width // n_tp
    cap = 3 * tokens * top // (2 * n_ep)
    cap = -(-cap // 8) * 8
    place = jnp.stack([lax.axis_index("tp"), lax.axis_index("ep")]).astype(jnp.int32)
    half = n_ep // 2

    weights = {0: mix_out_weight}
    for k in range(2, n_tp, 2):
        weights[k] = send(mix_out_weight, "tp", k)
    for k in range(0, n_tp, 2):
        weights[k + 1] = send(weights[k], "tp", 1)

    qt, kvt = prep(
        place,
        *map(far_memory, (queries, key_input, value_input, query_gain[None], key_gain[None], table)),
        heads,
    )
    blocks = [kvt]
    blocks += [send(kvt, "ep", k) for k in range(n_ep - 2, 0, -2)]
    blocks.append(send(kvt, "ep", 1))
    blocks += [send(b, "ep", 1) for b in blocks[1:half]]

    outbound, slot = dispatch(place, far_memory(routes.T), far_memory(expert_input), n_ep, cap, feat)
    arrived = lax.all_to_all(outbound, "ep", split_axis=0, concat_axis=0, tiled=True)
    xs = {0: arrived}
    for k in range(2, n_tp, 2):
        xs[k] = send(arrived, "tp", k)
    for k in range(0, n_tp, 2):
        xs[k + 1] = send(xs[k], "tp", 1)

    atts = attend(place, far_memory(qt), blocks, heads, n_tp)
    atts = [atts[0]] + [send(atts[k], "tp", k) for k in range(1, n_tp)]

    parts = expert(
        place, [xs[k] for k in range(n_tp)], far_memory(ffn_gain[None]), gate_weight[0], up_weight[0], down_weight[0], n_ep
    )
    returned = []
    for side in range(2):
        mine = {k: (parts[2 * k + side], send(parts[2 * k + 2 + side], "tp", 1)) for k in range(0, n_tp, 2)}
        terms = list(mine[0])
        for k in range(2, n_tp, 2):
            (both,) = finish(place, mine[k], 1)
            terms.append(send(both, "tp", k))
        pieces = finish(place, terms, half)
        for i, piece in enumerate(pieces):
            k = i ^ half if side == 0 else i
            returned.append(send(piece, "ep", k) if k else piece)

    mixed = mix(place, atts, [weights[k] for k in range(n_tp)])
    out = combine(place, slot, far_memory(route_scores.T), returned)
    return mixed, out


def solution(mesh):
    n_ep = mesh.shape["ep"]
    placed = (
        P(),
        P("ep", "tp"),
        P("ep", None),
        P("ep", None),
        P(),
        P(),
        P("tp", None),
        P("ep", None),
        P(),
        P("ep", None),
        P("ep", None),
        P("ep", None, "tp"),
        P("ep", None, "tp"),
        P("ep", "tp", None),
    )

    step = jax.shard_map(
        local,
        mesh=mesh,
        in_specs=placed,
        out_specs=(P(("ep", "tp"), None), P("ep", "tp")),
        check_vma=False,
    )

    def run(queries, *rest):
        table = jnp.asarray(rope_tables(queries.shape[0] // n_ep, n_ep))
        return step(table, queries, *rest)

    return run
```

```python
import functools

import jax
import jax.numpy as jnp
import numpy as np
from jax import lax
from jax.experimental import pallas as pl
from jax.experimental.pallas import tpu as pltpu
from jax.sharding import PartitionSpec as P


HEADS = 16
KV_HEADS = 4
HD = 64
GRID_W = 64
EPSILON = 1e-06
ROPE_BASE = 10000.0
LOG2E = 1.4426950408889634
F32 = jnp.float32
BF16 = jnp.bfloat16
VMEM_LIMIT = 24 * 1024 * 1024
FLOPS_PER_MICRO = 500_000_000


def full(shape):
    return pl.BlockSpec(shape, lambda *_: (0,) * len(shape))


def hbm():
    return pl.BlockSpec(memory_space=pltpu.HBM)


def far_memory(x):
    return pltpu.with_memory_space_constraint(x, pltpu.HBM)


def call(body, place, args, in_specs, outs, grid=(1,), scratch=(), out_specs=None, micros=1.0):
    return pl.pallas_call(
        body,
        grid_spec=pltpu.PrefetchScalarGridSpec(
            num_scalar_prefetch=1,
            grid=grid,
            in_specs=in_specs,
            out_specs=[full(o.shape) for o in outs] if out_specs is None else out_specs,
            scratch_shapes=list(scratch),
        ),
        out_shape=outs,
        cost_estimate=pl.CostEstimate(
            flops=int(micros * FLOPS_PER_MICRO), transcendentals=0, bytes_accessed=0
        ),
        compiler_params=pltpu.CompilerParams(
            dimension_semantics=("arbitrary",) * len(grid), vmem_limit_bytes=VMEM_LIMIT
        ),
    )(place, *args)


def mm(a, b, dims=((1,), (0,))):
    return lax.dot_general(a, b, (dims, ((), ())), preferred_element_type=F32)


def send(x, axis, flip):
    n = lax.axis_size(axis)
    return lax.ppermute(x, axis, [(i, i ^ flip) for i in range(n)])


def dispatch_body(place, routes_ref, x_hbm, *outs, experts, cap):
    out_ref, slot_ref, x_ref, sem = outs
    tokens, feat = x_ref.shape
    cols = pl.ds(pl.multiple_of(place[0] * feat, feat), feat)
    fetch = pltpu.make_async_copy(x_hbm.at[:, cols], x_ref, sem)
    fetch.start()
    routes = routes_ref[...]
    rows = lax.broadcasted_iota(jnp.int32, (experts, tokens), 0)
    first = (rows == routes[0:1, :]).astype(F32)
    second = (rows == routes[1:2, :]).astype(F32)
    hits = first + second
    row = lax.broadcasted_iota(jnp.int32, (tokens, tokens), 0)
    col = lax.broadcasted_iota(jnp.int32, (tokens, tokens), 1)
    before = (row < col).astype(F32).astype(BF16)
    count = mm(hits.astype(BF16), before)
    slot = jnp.where(hits > 0.5, count, -1.0).astype(jnp.int32)

    def flat(choice, expert):
        at = jnp.sum(count * choice, axis=0, keepdims=True).astype(jnp.int32)
        return (expert ^ place[1] ^ (experts // 2)) * cap + at

    slot_ref[0:1, :] = flat(first, routes[0:1, :])
    slot_ref[1:2, :] = flat(second, routes[1:2, :])
    fetch.wait()
    x = x_ref[...]
    slots = lax.broadcasted_iota(jnp.int32, (cap, tokens), 0)
    picks = [(slots == slot[e : e + 1, :]).astype(F32) for e in range(experts)]
    out_ref[...] = mm(jnp.concatenate(picks, axis=0).astype(BF16), x).astype(BF16)


def dispatch(place, routes, expert_input, experts, cap, feat):
    tokens = routes.shape[1]
    outs = [jax.ShapeDtypeStruct((experts * cap, feat), BF16), jax.ShapeDtypeStruct((2, tokens), jnp.int32)]
    return call(
        functools.partial(dispatch_body, experts=experts, cap=cap),
        place,
        (routes, expert_input),
        [full(routes.shape), hbm()],
        outs,
        scratch=[pltpu.VMEM((tokens, feat), BF16), pltpu.SemaphoreType.DMA],
        micros=1.5,
    )


def rope_tables(token_count, n_ep):
    quarter = HD // 4
    inverse = (np.float32(ROPE_BASE) ** (-np.arange(quarter, dtype=np.float32) / np.float32(quarter))).astype(
        np.float32
    )
    pos = np.arange(token_count * n_ep)

    def both(steps):
        angle = (inverse[:, None] * steps.astype(np.float32)[None, :]).astype(np.float32).astype(np.float64)
        return np.concatenate([np.cos(angle), np.sin(angle)], 0).astype(np.float32)

    return np.concatenate([both(pos // GRID_W), both(pos % GRID_W)], 0)


def turn(x, gain, table, low):
    quarter = HD // 4
    x = x.astype(F32)
    scale = lax.rsqrt(jnp.mean(x * x, axis=0, keepdims=True) + EPSILON)
    x = x * scale * gain
    u0, w0, u1, w1 = (x[i * quarter : (i + 1) * quarter] for i in range(4))
    cr, sr, cc, sc = (table[i * quarter : (i + 1) * quarter] for i in range(4))
    return jnp.concatenate(
        [u0 * cr - w0 * sr, w0 * cr + u0 * sr, u1 * cc - w1 * sc, w1 * cc + u1 * sc], axis=0
    ).astype(low)


def column(row):
    n = row.shape[1]
    same = lax.broadcasted_iota(jnp.int32, (n, n), 0) == lax.broadcasted_iota(jnp.int32, (n, n), 1)
    return jnp.sum(jnp.where(same, row, 0.0), axis=1, keepdims=True)


def prep_body(
    place,
    q_hbm,
    k_hbm,
    v_hbm,
    q_gain_ref,
    k_gain_ref,
    table_hbm,
    qt_ref,
    kvt_ref,
    turned_ref,
    q_ref,
    k_ref,
    v_ref,
    table_ref,
    sems,
    *,
    heads,
    group,
):
    rows = q_ref.shape[0]
    cols = pl.ds(pl.multiple_of(place[1] * rows, rows), rows)
    copies = [
        pltpu.make_async_copy(src, dst, sems.at[i])
        for i, (src, dst) in enumerate(
            ((k_hbm, k_ref), (table_hbm.at[:, cols], table_ref), (v_hbm, v_ref), (q_hbm, q_ref))
        )
    ]
    for c in copies:
        c.start()
    for c in copies:
        c.wait()
    table = table_ref[...]
    q_gain = column(q_gain_ref[...])
    k_gain = column(k_gain_ref[...])
    qt = q_ref[...].astype(F32).T
    for h in range(heads):
        qt_ref[h * HD : (h + 1) * HD, :] = turn(qt[h * HD : (h + 1) * HD], q_gain, table, BF16)
    start = pl.multiple_of((place[0] * heads // group) * HD, HD)
    turned_ref[...] = k_ref[...].astype(F32).T
    kvt_ref[:HD, :] = turn(turned_ref[pl.ds(start, HD), :], k_gain, table, BF16)
    turned_ref[...] = v_ref[...].astype(F32).T
    kvt_ref[HD:, :] = turned_ref[pl.ds(start, HD), :].astype(BF16)


def prep(place, queries, key_input, value_input, q_gain, k_gain, table, heads):
    rows = queries.shape[0]
    return call(
        functools.partial(prep_body, heads=heads, group=HEADS // KV_HEADS),
        place,
        (queries, key_input, value_input, q_gain, k_gain, table),
        [
            hbm(),
            hbm(),
            hbm(),
            full(q_gain.shape),
            full(k_gain.shape),
            hbm(),
        ],
        [
            pltpu.HBM((queries.shape[1], rows), BF16),
            jax.ShapeDtypeStruct((2 * HD, rows), BF16),
        ],
        scratch=[
            pltpu.VMEM((key_input.shape[1], rows), F32),
            pltpu.VMEM(queries.shape, BF16),
            pltpu.VMEM(key_input.shape, BF16),
            pltpu.VMEM(value_input.shape, BF16),
            pltpu.VMEM((table.shape[0], rows), F32),
            pltpu.SemaphoreType.DMA((4,)),
        ],
        micros=2.0,
    )


def attend_body(place, qt_ref, *refs, blocks, heads, count, groups):
    if groups:
        num_in, den_in = refs[:2]
        refs = refs[2:]
        kv_refs, out_refs = refs[:count], refs[count : count + groups]
        out_ref, k_ref, v_ref, num_ref, den_ref = refs[count + groups :]
        num_ref[...] = num_in[...]
        den_ref[...] = den_in[...]
    else:
        kv_refs, (num_ref, den_ref, k_ref, v_ref) = refs[:count], refs[count:]
        num_ref[...] = jnp.zeros_like(num_ref)
        den_ref[...] = jnp.zeros_like(den_ref)
    keys = kv_refs[0].shape[1]
    for b in range(blocks):
        k_ref[b] = kv_refs[b][:HD, :].astype(F32).T.astype(BF16)
        v_ref[b] = kv_refs[b][HD:, :]

    def one(b, carry):
        k = k_ref[b]
        v = v_ref[b]
        for h in range(heads):
            q = qt_ref[h * HD : (h + 1) * HD, :]
            p = jnp.exp2(mm(k, q) * (LOG2E * HD**-0.5))
            den_ref[h * 8 : (h + 1) * 8, :] += jnp.sum(p.reshape(keys // 8, 8, p.shape[1]), axis=0)
            num_ref[h * HD : (h + 1) * HD, :] += mm(v, p.astype(BF16))
        return carry

    lax.fori_loop(0, blocks, one, 0)
    if groups:
        for h in range(heads):
            den = jnp.sum(den_ref[h * 8 : (h + 1) * 8, :], axis=0, keepdims=True)
            num_ref[h * HD : (h + 1) * HD, :] = num_ref[h * HD : (h + 1) * HD, :] / den
        out_ref[...] = num_ref[...].T
        rows = out_refs[0].shape[0]
        for k in range(groups):
            at = pl.multiple_of((place[0] ^ k) * rows, rows)
            out_refs[k][...] = out_ref[pl.ds(at, rows), :].astype(BF16)


def attend(place, qt, sums, kv_blocks, heads, groups):
    rows = qt.shape[1]
    keys = kv_blocks[0].shape[1]
    count = len(kv_blocks)
    held = [pltpu.HBM(qt.shape, F32), pltpu.HBM((heads * 8, rows), F32)]
    scratch = [pltpu.VMEM((count, keys, HD), BF16), pltpu.VMEM((count, HD, keys), BF16)]
    if groups:
        outs = [jax.ShapeDtypeStruct((rows // groups, qt.shape[0]), BF16)] * groups
        scratch = [pltpu.VMEM((rows, qt.shape[0]), F32)] + scratch + [pltpu.VMEM(h.shape, F32) for h in held]
    else:
        outs = held
    return call(
        functools.partial(attend_body, blocks=count, heads=heads, count=count, groups=groups),
        place,
        (qt, *sums, *kv_blocks),
        [full(qt.shape)] + [full(x.shape) for x in sums] + [full(b.shape) for b in kv_blocks],
        outs,
        scratch=scratch,
        micros=7.0,
    )


def mix_body(place, *refs, groups):
    att_refs, w_refs, out_ref = refs[:groups], refs[groups : 2 * groups], refs[2 * groups]
    total = jnp.zeros(out_ref.shape, F32)
    for k in range(groups):
        total += mm(att_refs[k][...], w_refs[k][...]).astype(BF16).astype(F32)
    out_ref[...] = total.astype(BF16)


def mix(place, atts, weights):
    groups = len(weights)
    rows = atts[0].shape[0]
    depth, width = weights[0].shape
    tile = min(width, 512)
    return call(
        functools.partial(mix_body, groups=groups),
        place,
        (*atts, *weights),
        [full(a.shape) for a in atts] + [pl.BlockSpec((depth, tile), lambda j, place: (0, j))] * groups,
        [jax.ShapeDtypeStruct((rows, width), BF16)],
        grid=(width // tile,),
        out_specs=[pl.BlockSpec((rows, tile), lambda j, place: (0, j))],
        micros=2.5,
    )[0]


def expert_body(place, *refs, groups, tile, experts):
    x_refs = refs[:groups]
    gain_ref, gate_ref, up_ref, down_ref = refs[groups : groups + 4]
    out_refs = refs[groups + 4 : 3 * groups + 4]
    scaled_ref, hidden_ref = refs[3 * groups + 4 :]
    rows, feat = x_refs[0].shape
    cap = rows // experts
    half = rows // 2
    width = groups * feat

    def spot(k):
        return pl.ds(pl.multiple_of((place[0] ^ k) * feat, feat), feat)

    parts = []
    for i in range(experts):
        at = pl.multiple_of((place[1] ^ i ^ (experts // 2)) * cap, cap)
        squares = 0.0
        for k in range(groups):
            x = x_refs[k][pl.ds(at, cap), :].astype(F32)
            scaled_ref[i * cap : (i + 1) * cap, spot(k)] = (x * gain_ref[:, spot(k)]).astype(BF16)
            squares += x * x
        parts.append(jnp.sum(squares, axis=1, keepdims=True))
    scale = lax.rsqrt(jnp.concatenate(parts, axis=0) / width + EPSILON)

    for j in range(gate_ref.shape[1] // tile):
        x = scaled_ref[...]
        cols = slice(j * tile, (j + 1) * tile)
        gate = mm(x, gate_ref[:, cols]) * scale
        up = mm(x, up_ref[:, cols]) * scale
        hidden_ref[:, cols] = (gate / (1.0 + jnp.exp(-gate)) * up).astype(BF16)
    for k in range(groups):
        part = mm(hidden_ref[...], down_ref[:, spot(k)]).astype(BF16)
        out_refs[2 * k][...] = part[:half]
        out_refs[2 * k + 1][...] = part[half:]


def expert(place, xs, gain, gate, up, down, experts):
    groups = len(xs)
    rows, feat = xs[0].shape
    depth, ff = gate.shape
    tile = min(ff, 256)
    vmem = pl.BlockSpec(memory_space=pltpu.VMEM)
    return call(
        functools.partial(expert_body, groups=groups, tile=tile, experts=experts),
        place,
        (*xs, gain, gate, up, down),
        [full(x.shape) for x in xs] + [full(gain.shape), vmem, vmem, vmem],
        [jax.ShapeDtypeStruct((rows // 2, feat), BF16)] * (2 * groups),
        scratch=[pltpu.VMEM((rows, depth), BF16), pltpu.VMEM((rows, ff), BF16)],
        micros=9.0,
    )


def combine_body(place, slot_ref, scores_ref, *refs, blocks):
    out_ref, rows_ref = refs[blocks:]
    tokens = out_ref.shape[0]
    cap = refs[0].shape[0]
    for i in range(blocks):
        rows_ref[i * cap : (i + 1) * cap, :] = refs[i][...]
    scores = scores_ref[...]
    weight = scores / jnp.sum(scores, axis=0, keepdims=True)
    slot = slot_ref[...]
    rows = lax.broadcasted_iota(jnp.int32, (blocks * cap, tokens), 0)
    total = jnp.zeros(out_ref.shape, F32)
    for k in range(2):
        pick = (rows == slot[k : k + 1, :]).astype(F32).astype(BF16)
        total += mm(pick, rows_ref[...], ((0,), (0,))) * column(weight[k : k + 1, :])
    out_ref[...] = total.astype(BF16)


def combine(place, slot, scores, rows):
    cap, feat = rows[0].shape
    return call(
        functools.partial(combine_body, blocks=len(rows)),
        place,
        (slot, scores, *rows),
        [full(slot.shape), full(scores.shape)] + [full(r.shape) for r in rows],
        [jax.ShapeDtypeStruct((slot.shape[1], feat), BF16)],
        scratch=[pltpu.VMEM((len(rows) * cap, feat), BF16)],
        micros=1.5,
    )[0]


def local(
    table,
    queries,
    key_input,
    value_input,
    query_gain,
    key_gain,
    mix_out_weight,
    expert_input,
    ffn_gain,
    routes,
    route_scores,
    gate_weight,
    up_weight,
    down_weight,
):
    n_ep = lax.axis_size("ep")
    n_tp = lax.axis_size("tp")
    heads = queries.shape[1] // HD
    tokens, top = routes.shape
    width = expert_input.shape[1]
    feat = width // n_tp
    cap = 3 * tokens * top // (2 * n_ep)
    cap = -(-cap // 8) * 8
    place = jnp.stack([lax.axis_index("tp"), lax.axis_index("ep")]).astype(jnp.int32)
    half = n_ep // 2

    weights = {0: mix_out_weight}
    for k in range(2, n_tp, 2):
        weights[k] = send(mix_out_weight, "tp", k)
    for k in range(0, n_tp, 2):
        weights[k + 1] = send(weights[k], "tp", 1)

    qt, kvt = prep(
        place,
        *map(far_memory, (queries, key_input, value_input, query_gain[None], key_gain[None], table)),
        heads,
    )
    blocks = [kvt]
    blocks += [send(kvt, "ep", k) for k in range(n_ep - 2, 0, -2)]
    blocks.append(send(kvt, "ep", 1))
    blocks += [send(b, "ep", 1) for b in blocks[1:half]]

    outbound, slot = dispatch(place, far_memory(routes.T), far_memory(expert_input), n_ep, cap, feat)
    arrived = lax.all_to_all(outbound, "ep", split_axis=0, concat_axis=0, tiled=True)
    xs = {0: arrived}
    for k in range(2, n_tp, 2):
        xs[k] = send(arrived, "tp", k)
    for k in range(0, n_tp, 2):
        xs[k + 1] = send(xs[k], "tp", 1)

    sums = attend(place, far_memory(qt), (), blocks[:half], heads, 0)
    atts = attend(place, far_memory(qt), [far_memory(x) for x in sums], blocks[half:], heads, n_tp)
    atts = [atts[0]] + [send(atts[k], "tp", k) for k in range(1, n_tp)]

    parts = expert(
        place, [xs[k] for k in range(n_tp)], far_memory(ffn_gain[None]), gate_weight[0], up_weight[0], down_weight[0], n_ep
    )
    returned = []
    for side in range(2):
        mine = {k: (parts[2 * k + side], send(parts[2 * k + 2 + side], "tp", 1)) for k in range(0, n_tp, 2)}
        terms = list(mine[0])
        for k in range(2, n_tp, 2):
            both = (mine[k][0].astype(F32) + mine[k][1].astype(F32)).astype(BF16)
            terms.append(send(both, "tp", k))
        for i in range(half):
            piece = sum(t[i * cap : (i + 1) * cap].astype(F32) for t in terms).astype(BF16)
            k = i ^ half if side == 0 else i
            returned.append(send(piece, "ep", k) if k else piece)

    mixed = mix(place, atts, [weights[k] for k in range(n_tp)])
    out = combine(place, slot, route_scores.T, returned)
    return mixed, out


def solution(mesh):
    n_ep = mesh.shape["ep"]
    placed = (
        P(),
        P("ep", "tp"),
        P("ep", None),
        P("ep", None),
        P(),
        P(),
        P("tp", None),
        P("ep", None),
        P(),
        P("ep", None),
        P("ep", None),
        P("ep", None, "tp"),
        P("ep", None, "tp"),
        P("ep", "tp", None),
    )

    step = jax.shard_map(
        local,
        mesh=mesh,
        in_specs=placed,
        out_specs=(P(("ep", "tp"), None), P("ep", "tp")),
        check_vma=False,
    )

    def run(queries, *rest):
        table = jnp.asarray(rope_tables(queries.shape[0] // n_ep, n_ep))
        return step(table, queries, *rest)

    return run
```

```python
import functools

import jax
import jax.numpy as jnp
import numpy as np
from jax import lax
from jax.experimental import pallas as pl
from jax.experimental.pallas import tpu as pltpu
from jax.sharding import PartitionSpec as P


HEADS = 16
KV_HEADS = 4
HD = 64
GRID_W = 64
EPSILON = 1e-06
ROPE_BASE = 10000.0
LOG2E = 1.4426950408889634
F32 = jnp.float32
BF16 = jnp.bfloat16
VMEM_LIMIT = 24 * 1024 * 1024
FLOPS_PER_MICRO = 500_000_000
SPAN = 4


def full(shape):
    return pl.BlockSpec(shape, lambda *_: (0,) * len(shape))


def hbm():
    return pl.BlockSpec(memory_space=pltpu.HBM)


def far_memory(x):
    return pltpu.with_memory_space_constraint(x, pltpu.HBM)


def call(body, place, args, in_specs, outs, grid=(1,), scratch=(), out_specs=None, micros=1.0):
    return pl.pallas_call(
        body,
        grid_spec=pltpu.PrefetchScalarGridSpec(
            num_scalar_prefetch=1,
            grid=grid,
            in_specs=in_specs,
            out_specs=[full(o.shape) for o in outs] if out_specs is None else out_specs,
            scratch_shapes=list(scratch),
        ),
        out_shape=outs,
        cost_estimate=pl.CostEstimate(
            flops=int(micros * FLOPS_PER_MICRO), transcendentals=0, bytes_accessed=0
        ),
        compiler_params=pltpu.CompilerParams(
            dimension_semantics=("arbitrary",) * len(grid), vmem_limit_bytes=VMEM_LIMIT
        ),
    )(place, *args)


def mm(a, b, dims=((1,), (0,))):
    return lax.dot_general(a, b, (dims, ((), ())), preferred_element_type=F32)


def send(x, axis, flip):
    n = lax.axis_size(axis)
    return lax.ppermute(x, axis, [(i, i ^ flip) for i in range(n)])


def dispatch_body(place, routes_ref, x_hbm, *outs, experts, cap):
    out_ref, slot_ref, x_ref, sem = outs
    tokens, feat = x_ref.shape
    cols = pl.ds(pl.multiple_of(place[0] * feat, feat), feat)
    fetch = pltpu.make_async_copy(x_hbm.at[:, cols], x_ref, sem)
    fetch.start()
    routes = routes_ref[...]
    rows = lax.broadcasted_iota(jnp.int32, (experts, tokens), 0)
    first = (rows == routes[0:1, :]).astype(F32)
    second = (rows == routes[1:2, :]).astype(F32)
    hits = first + second
    row = lax.broadcasted_iota(jnp.int32, (tokens, tokens), 0)
    col = lax.broadcasted_iota(jnp.int32, (tokens, tokens), 1)
    before = (row < col).astype(F32).astype(BF16)
    count = mm(hits.astype(BF16), before)
    slot = jnp.where(hits > 0.5, count, -1.0).astype(jnp.int32)

    def flat(choice, expert):
        at = jnp.sum(count * choice, axis=0, keepdims=True).astype(jnp.int32)
        return (expert ^ place[1] ^ (experts // 2)) * cap + at

    slot_ref[0:1, :] = flat(first, routes[0:1, :])
    slot_ref[1:2, :] = flat(second, routes[1:2, :])
    fetch.wait()
    x = x_ref[...]
    slots = lax.broadcasted_iota(jnp.int32, (cap, tokens), 0)
    picks = [(slots == slot[e : e + 1, :]).astype(F32) for e in range(experts)]
    out_ref[...] = mm(jnp.concatenate(picks, axis=0).astype(BF16), x).astype(BF16)


def dispatch(place, routes, expert_input, experts, cap, feat):
    tokens = routes.shape[1]
    outs = [jax.ShapeDtypeStruct((experts * cap, feat), BF16), jax.ShapeDtypeStruct((2, tokens), jnp.int32)]
    return call(
        functools.partial(dispatch_body, experts=experts, cap=cap),
        place,
        (routes, expert_input),
        [full(routes.shape), hbm()],
        outs,
        scratch=[pltpu.VMEM((tokens, feat), BF16), pltpu.SemaphoreType.DMA],
        micros=1.5,
    )


def rope_tables(token_count, n_ep):
    quarter = HD // 4
    inverse = (np.float32(ROPE_BASE) ** (-np.arange(quarter, dtype=np.float32) / np.float32(quarter))).astype(
        np.float32
    )
    pos = np.arange(token_count * n_ep)

    def both(steps):
        angle = (inverse[:, None] * steps.astype(np.float32)[None, :]).astype(np.float32).astype(np.float64)
        return np.concatenate([np.cos(angle), np.sin(angle)], 0).astype(np.float32)

    return np.concatenate([both(pos // GRID_W), both(pos % GRID_W)], 0)


def turn(x, gain, table, low):
    quarter = HD // 4
    x = x.astype(F32)
    scale = lax.rsqrt(jnp.mean(x * x, axis=0, keepdims=True) + EPSILON)
    x = x * scale * gain
    u0, w0, u1, w1 = (x[i * quarter : (i + 1) * quarter] for i in range(4))
    cr, sr, cc, sc = (table[i * quarter : (i + 1) * quarter] for i in range(4))
    return jnp.concatenate(
        [u0 * cr - w0 * sr, w0 * cr + u0 * sr, u1 * cc - w1 * sc, w1 * cc + u1 * sc], axis=0
    ).astype(low)


def column(row):
    n = row.shape[1]
    same = lax.broadcasted_iota(jnp.int32, (n, n), 0) == lax.broadcasted_iota(jnp.int32, (n, n), 1)
    return jnp.sum(jnp.where(same, row, 0.0), axis=1, keepdims=True)


def prep_body(
    place,
    q_hbm,
    k_hbm,
    v_hbm,
    q_gain_ref,
    k_gain_ref,
    table_hbm,
    qt_ref,
    kvt_ref,
    turned_ref,
    q_ref,
    k_ref,
    v_ref,
    table_ref,
    sems,
    *,
    heads,
    group,
):
    rows = q_ref.shape[0]
    cols = pl.ds(pl.multiple_of(place[1] * rows, rows), rows)
    copies = [
        pltpu.make_async_copy(src, dst, sems.at[i])
        for i, (src, dst) in enumerate(
            ((k_hbm, k_ref), (table_hbm.at[:, cols], table_ref), (v_hbm, v_ref), (q_hbm, q_ref))
        )
    ]
    for c in copies:
        c.start()
    for c in copies:
        c.wait()
    table = table_ref[...]
    q_gain = column(q_gain_ref[...])
    k_gain = column(k_gain_ref[...])
    qt = q_ref[...].astype(F32).T
    for h in range(heads):
        qt_ref[h * HD : (h + 1) * HD, :] = turn(qt[h * HD : (h + 1) * HD], q_gain, table, BF16)
    start = pl.multiple_of((place[0] * heads // group) * HD, HD)
    turned_ref[...] = k_ref[...].astype(F32).T
    kvt_ref[:HD, :] = turn(turned_ref[pl.ds(start, HD), :], k_gain, table, BF16)
    turned_ref[...] = v_ref[...].astype(F32).T
    kvt_ref[HD:, :] = turned_ref[pl.ds(start, HD), :].astype(BF16)


def prep(place, queries, key_input, value_input, q_gain, k_gain, table, heads):
    rows = queries.shape[0]
    return call(
        functools.partial(prep_body, heads=heads, group=HEADS // KV_HEADS),
        place,
        (queries, key_input, value_input, q_gain, k_gain, table),
        [
            hbm(),
            hbm(),
            hbm(),
            full(q_gain.shape),
            full(k_gain.shape),
            hbm(),
        ],
        [
            pltpu.HBM((queries.shape[1], rows), BF16),
            jax.ShapeDtypeStruct((2 * HD, rows), BF16),
        ],
        scratch=[
            pltpu.VMEM((key_input.shape[1], rows), F32),
            pltpu.VMEM(queries.shape, BF16),
            pltpu.VMEM(key_input.shape, BF16),
            pltpu.VMEM(value_input.shape, BF16),
            pltpu.VMEM((table.shape[0], rows), F32),
            pltpu.SemaphoreType.DMA((4,)),
        ],
        micros=2.0,
    )


def attend_body(place, qt_ref, *refs, heads, count, groups):
    sums = refs[: len(refs) - count - 4 - (groups + 1 if groups else 0)]
    refs = refs[len(sums) :]
    if groups:
        kv_refs, out_refs = refs[:count], refs[count : count + groups]
        out_ref, k_ref, v_ref, num_ref, den_ref = refs[count + groups :]
    else:
        kv_refs, (num_ref, den_ref, k_ref, v_ref) = refs[:count], refs[count:]
    num_ref[...] = sums[0][...] if sums else jnp.zeros_like(num_ref)
    den_ref[...] = sums[1][...] if sums else jnp.zeros_like(den_ref)
    keys = kv_refs[0].shape[1]
    for b in range(count):
        k_ref[b * keys : (b + 1) * keys, :] = kv_refs[b][:HD, :].astype(F32).T.astype(BF16)
        v_ref[:, b * keys : (b + 1) * keys] = kv_refs[b][HD:, :]
    for b in range(0, count, SPAN):
        at = slice(b * keys, min(b + SPAN, count) * keys)
        for h in range(heads):
            q = qt_ref[h * HD : (h + 1) * HD, :]
            p = jnp.exp2(mm(k_ref[at, :], q) * (LOG2E * HD**-0.5))
            den_ref[h * 8 : (h + 1) * 8, :] += jnp.sum(p.reshape(p.shape[0] // 8, 8, p.shape[1]), axis=0)
            num_ref[h * HD : (h + 1) * HD, :] += mm(v_ref[:, at], p.astype(BF16))
    if groups:
        for h in range(heads):
            den = jnp.sum(den_ref[h * 8 : (h + 1) * 8, :], axis=0, keepdims=True)
            num_ref[h * HD : (h + 1) * HD, :] = num_ref[h * HD : (h + 1) * HD, :] / den
        out_ref[...] = num_ref[...].T
        rows = out_refs[0].shape[0]
        for k in range(groups):
            at = pl.multiple_of((place[0] ^ k) * rows, rows)
            out_refs[k][...] = out_ref[pl.ds(at, rows), :].astype(BF16)


def attend(place, qt, sums, kv_blocks, heads, groups):
    rows = qt.shape[1]
    keys = kv_blocks[0].shape[1]
    count = len(kv_blocks)
    held = [pltpu.HBM(qt.shape, F32), pltpu.HBM((heads * 8, rows), F32)]
    scratch = [pltpu.VMEM((count * keys, HD), BF16), pltpu.VMEM((HD, count * keys), BF16)]
    if groups:
        outs = [jax.ShapeDtypeStruct((rows // groups, qt.shape[0]), BF16)] * groups
        scratch = [pltpu.VMEM((rows, qt.shape[0]), F32)] + scratch + [pltpu.VMEM(h.shape, F32) for h in held]
    else:
        outs = held
    return call(
        functools.partial(attend_body, heads=heads, count=count, groups=groups),
        place,
        (qt, *sums, *kv_blocks),
        [full(qt.shape)] + [full(x.shape) for x in sums] + [full(b.shape) for b in kv_blocks],
        outs,
        scratch=scratch,
        micros=1.4 * count,
    )


def mix_body(place, *refs, groups):
    att_refs, w_refs, out_ref = refs[:groups], refs[groups : 2 * groups], refs[2 * groups]
    total = jnp.zeros(out_ref.shape, F32)
    for k in range(groups):
        total += mm(att_refs[k][...], w_refs[k][...]).astype(BF16).astype(F32)
    out_ref[...] = total.astype(BF16)


def mix(place, atts, weights):
    groups = len(weights)
    rows = atts[0].shape[0]
    depth, width = weights[0].shape
    tile = min(width, 512)
    return call(
        functools.partial(mix_body, groups=groups),
        place,
        (*atts, *weights),
        [full(a.shape) for a in atts] + [pl.BlockSpec((depth, tile), lambda j, place: (0, j))] * groups,
        [jax.ShapeDtypeStruct((rows, width), BF16)],
        grid=(width // tile,),
        out_specs=[pl.BlockSpec((rows, tile), lambda j, place: (0, j))],
        micros=2.5,
    )[0]


def expert_body(place, *refs, groups, tile, experts):
    x_refs = refs[:groups]
    gain_ref, gate_ref, up_ref, down_ref = refs[groups : groups + 4]
    out_refs = refs[groups + 4 : 3 * groups + 4]
    scaled_ref, hidden_ref = refs[3 * groups + 4 :]
    rows, feat = x_refs[0].shape
    cap = rows // experts
    half = rows // 2
    width = groups * feat

    def spot(k):
        return pl.ds(pl.multiple_of((place[0] ^ k) * feat, feat), feat)

    parts = []
    for i in range(experts):
        at = pl.multiple_of((place[1] ^ i ^ (experts // 2)) * cap, cap)
        squares = 0.0
        for k in range(groups):
            x = x_refs[k][pl.ds(at, cap), :].astype(F32)
            scaled_ref[i * cap : (i + 1) * cap, spot(k)] = (x * gain_ref[:, spot(k)]).astype(BF16)
            squares += x * x
        parts.append(jnp.sum(squares, axis=1, keepdims=True))
    scale = lax.rsqrt(jnp.concatenate(parts, axis=0) / width + EPSILON)

    for j in range(gate_ref.shape[1] // tile):
        x = scaled_ref[...]
        cols = slice(j * tile, (j + 1) * tile)
        gate = mm(x, gate_ref[:, cols]) * scale
        up = mm(x, up_ref[:, cols]) * scale
        hidden_ref[:, cols] = (gate / (1.0 + jnp.exp(-gate)) * up).astype(BF16)
    for k in range(groups):
        part = mm(hidden_ref[...], down_ref[:, spot(k)]).astype(BF16)
        out_refs[2 * k][...] = part[:half]
        out_refs[2 * k + 1][...] = part[half:]


def expert(place, xs, gain, gate, up, down, experts):
    groups = len(xs)
    rows, feat = xs[0].shape
    depth, ff = gate.shape
    tile = min(ff, 256)
    vmem = pl.BlockSpec(memory_space=pltpu.VMEM)
    return call(
        functools.partial(expert_body, groups=groups, tile=tile, experts=experts),
        place,
        (*xs, gain, gate, up, down),
        [full(x.shape) for x in xs] + [full(gain.shape), vmem, vmem, vmem],
        [jax.ShapeDtypeStruct((rows // 2, feat), BF16)] * (2 * groups),
        scratch=[pltpu.VMEM((rows, depth), BF16), pltpu.VMEM((rows, ff), BF16)],
        micros=9.0,
    )


def combine_body(place, slot_ref, scores_ref, *refs, blocks):
    out_ref, rows_ref = refs[blocks:]
    tokens = out_ref.shape[0]
    cap = refs[0].shape[0]
    for i in range(blocks):
        rows_ref[i * cap : (i + 1) * cap, :] = refs[i][...]
    scores = scores_ref[...]
    weight = scores / jnp.sum(scores, axis=0, keepdims=True)
    slot = slot_ref[...]
    rows = lax.broadcasted_iota(jnp.int32, (blocks * cap, tokens), 0)
    total = jnp.zeros(out_ref.shape, F32)
    for k in range(2):
        pick = (rows == slot[k : k + 1, :]).astype(F32).astype(BF16)
        total += mm(pick, rows_ref[...], ((0,), (0,))) * column(weight[k : k + 1, :])
    out_ref[...] = total.astype(BF16)


def combine(place, slot, scores, rows):
    cap, feat = rows[0].shape
    return call(
        functools.partial(combine_body, blocks=len(rows)),
        place,
        (slot, scores, *rows),
        [full(slot.shape), full(scores.shape)] + [full(r.shape) for r in rows],
        [jax.ShapeDtypeStruct((slot.shape[1], feat), BF16)],
        scratch=[pltpu.VMEM((len(rows) * cap, feat), BF16)],
        micros=1.5,
    )[0]


def local(
    table,
    queries,
    key_input,
    value_input,
    query_gain,
    key_gain,
    mix_out_weight,
    expert_input,
    ffn_gain,
    routes,
    route_scores,
    gate_weight,
    up_weight,
    down_weight,
):
    n_ep = lax.axis_size("ep")
    n_tp = lax.axis_size("tp")
    heads = queries.shape[1] // HD
    tokens, top = routes.shape
    width = expert_input.shape[1]
    feat = width // n_tp
    cap = 3 * tokens * top // (2 * n_ep)
    cap = -(-cap // 8) * 8
    place = jnp.stack([lax.axis_index("tp"), lax.axis_index("ep")]).astype(jnp.int32)
    half = n_ep // 2

    weights = {0: mix_out_weight}
    for k in range(2, n_tp, 2):
        weights[k] = send(mix_out_weight, "tp", k)
    for k in range(0, n_tp, 2):
        weights[k + 1] = send(weights[k], "tp", 1)

    qt, kvt = prep(
        place,
        *map(far_memory, (queries, key_input, value_input, query_gain[None], key_gain[None], table)),
        heads,
    )
    along = [send(kvt, "ep", k) for k in range(n_ep - 2, 0, -2)]
    beside = send(kvt, "ep", 1)
    across = [send(b, "ep", 1) for b in along]

    outbound, slot = dispatch(place, far_memory(routes.T), far_memory(expert_input), n_ep, cap, feat)
    arrived = lax.all_to_all(outbound, "ep", split_axis=0, concat_axis=0, tiled=True)
    xs = {0: arrived}
    for k in range(2, n_tp, 2):
        xs[k] = send(arrived, "tp", k)
    for k in range(0, n_tp, 2):
        xs[k + 1] = send(xs[k], "tp", 1)

    qt = far_memory(qt)
    sums = attend(place, qt, (), [kvt, beside], heads, 0)
    sums = attend(place, qt, [far_memory(x) for x in sums], along, heads, 0)
    atts = attend(place, qt, [far_memory(x) for x in sums], across, heads, n_tp)
    atts = [atts[0]] + [send(atts[k], "tp", k) for k in range(1, n_tp)]

    parts = expert(
        place, [xs[k] for k in range(n_tp)], far_memory(ffn_gain[None]), gate_weight[0], up_weight[0], down_weight[0], n_ep
    )
    returned = []
    for side in range(2):
        mine = {k: (parts[2 * k + side], send(parts[2 * k + 2 + side], "tp", 1)) for k in range(0, n_tp, 2)}
        terms = list(mine[0])
        for k in range(2, n_tp, 2):
            both = (mine[k][0].astype(F32) + mine[k][1].astype(F32)).astype(BF16)
            terms.append(send(both, "tp", k))
        for i in range(half):
            piece = sum(t[i * cap : (i + 1) * cap].astype(F32) for t in terms).astype(BF16)
            k = i ^ half if side == 0 else i
            returned.append(send(piece, "ep", k) if k else piece)

    mixed = mix(place, atts, [weights[k] for k in range(n_tp)])
    out = combine(place, slot, route_scores.T, returned)
    return mixed, out


def solution(mesh):
    n_ep = mesh.shape["ep"]
    placed = (
        P(),
        P("ep", "tp"),
        P("ep", None),
        P("ep", None),
        P(),
        P(),
        P("tp", None),
        P("ep", None),
        P(),
        P("ep", None),
        P("ep", None),
        P("ep", None, "tp"),
        P("ep", None, "tp"),
        P("ep", "tp", None),
    )

    step = jax.shard_map(
        local,
        mesh=mesh,
        in_specs=placed,
        out_specs=(P(("ep", "tp"), None), P("ep", "tp")),
        check_vma=False,
    )

    def run(queries, *rest):
        table = jnp.asarray(rope_tables(queries.shape[0] // n_ep, n_ep))
        return step(table, queries, *rest)

    return run
```

```python
import functools

import jax
import jax.numpy as jnp
import numpy as np
from jax import lax
from jax.experimental import pallas as pl
from jax.experimental.pallas import tpu as pltpu
from jax.sharding import PartitionSpec as P


HEADS = 16
KV_HEADS = 4
HD = 64
GRID_W = 64
EPSILON = 1e-06
ROPE_BASE = 10000.0
LOG2E = 1.4426950408889634
F32 = jnp.float32
BF16 = jnp.bfloat16
VMEM_LIMIT = 24 * 1024 * 1024
FLOPS_PER_MICRO = 500_000_000
SPAN = 6


def full(shape):
    return pl.BlockSpec(shape, lambda *_: (0,) * len(shape))


def hbm():
    return pl.BlockSpec(memory_space=pltpu.HBM)


def far_memory(x):
    return pltpu.with_memory_space_constraint(x, pltpu.HBM)


def call(body, place, args, in_specs, outs, grid=(1,), scratch=(), out_specs=None, micros=1.0):
    return pl.pallas_call(
        body,
        grid_spec=pltpu.PrefetchScalarGridSpec(
            num_scalar_prefetch=1,
            grid=grid,
            in_specs=in_specs,
            out_specs=[full(o.shape) for o in outs] if out_specs is None else out_specs,
            scratch_shapes=list(scratch),
        ),
        out_shape=outs,
        cost_estimate=pl.CostEstimate(
            flops=int(micros * FLOPS_PER_MICRO), transcendentals=0, bytes_accessed=0
        ),
        compiler_params=pltpu.CompilerParams(
            dimension_semantics=("arbitrary",) * len(grid), vmem_limit_bytes=VMEM_LIMIT
        ),
    )(place, *args)


def mm(a, b, dims=((1,), (0,))):
    return lax.dot_general(a, b, (dims, ((), ())), preferred_element_type=F32)


def send(x, axis, flip):
    n = lax.axis_size(axis)
    return lax.ppermute(x, axis, [(i, i ^ flip) for i in range(n)])


def dispatch_body(place, routes_ref, x_hbm, *outs, experts, cap):
    out_ref, slot_ref, x_ref, sem = outs
    tokens, feat = x_ref.shape
    cols = pl.ds(pl.multiple_of(place[0] * feat, feat), feat)
    fetch = pltpu.make_async_copy(x_hbm.at[:, cols], x_ref, sem)
    fetch.start()
    routes = routes_ref[...]
    rows = lax.broadcasted_iota(jnp.int32, (experts, tokens), 0)
    first = (rows == routes[0:1, :]).astype(F32)
    second = (rows == routes[1:2, :]).astype(F32)
    hits = first + second
    row = lax.broadcasted_iota(jnp.int32, (tokens, tokens), 0)
    col = lax.broadcasted_iota(jnp.int32, (tokens, tokens), 1)
    before = (row < col).astype(F32).astype(BF16)
    count = mm(hits.astype(BF16), before)
    slot = jnp.where(hits > 0.5, count, -1.0).astype(jnp.int32)

    def flat(choice, expert):
        at = jnp.sum(count * choice, axis=0, keepdims=True).astype(jnp.int32)
        return (expert ^ place[1] ^ (experts // 2)) * cap + at

    slot_ref[0:1, :] = flat(first, routes[0:1, :])
    slot_ref[1:2, :] = flat(second, routes[1:2, :])
    fetch.wait()
    x = x_ref[...]
    slots = lax.broadcasted_iota(jnp.int32, (cap, tokens), 0)
    picks = [(slots == slot[e : e + 1, :]).astype(F32) for e in range(experts)]
    out_ref[...] = mm(jnp.concatenate(picks, axis=0).astype(BF16), x).astype(BF16)


def dispatch(place, routes, expert_input, experts, cap, feat):
    tokens = routes.shape[1]
    outs = [jax.ShapeDtypeStruct((experts * cap, feat), BF16), jax.ShapeDtypeStruct((2, tokens), jnp.int32)]
    return call(
        functools.partial(dispatch_body, experts=experts, cap=cap),
        place,
        (routes, expert_input),
        [full(routes.shape), hbm()],
        outs,
        scratch=[pltpu.VMEM((tokens, feat), BF16), pltpu.SemaphoreType.DMA],
        micros=1.5,
    )


def rope_tables(token_count, n_ep):
    quarter = HD // 4
    inverse = (np.float32(ROPE_BASE) ** (-np.arange(quarter, dtype=np.float32) / np.float32(quarter))).astype(
        np.float32
    )
    pos = np.arange(token_count * n_ep)

    def both(steps):
        angle = (inverse[:, None] * steps.astype(np.float32)[None, :]).astype(np.float32).astype(np.float64)
        return np.concatenate([np.cos(angle), np.sin(angle)], 0).astype(np.float32)

    return np.concatenate([both(pos // GRID_W), both(pos % GRID_W)], 0)


def turn(x, gain, table, low):
    quarter = HD // 4
    x = x.astype(F32)
    scale = lax.rsqrt(jnp.mean(x * x, axis=0, keepdims=True) + EPSILON)
    x = x * scale * gain
    u0, w0, u1, w1 = (x[i * quarter : (i + 1) * quarter] for i in range(4))
    cr, sr, cc, sc = (table[i * quarter : (i + 1) * quarter] for i in range(4))
    return jnp.concatenate(
        [u0 * cr - w0 * sr, w0 * cr + u0 * sr, u1 * cc - w1 * sc, w1 * cc + u1 * sc], axis=0
    ).astype(low)


def column(row):
    n = row.shape[1]
    same = lax.broadcasted_iota(jnp.int32, (n, n), 0) == lax.broadcasted_iota(jnp.int32, (n, n), 1)
    return jnp.sum(jnp.where(same, row, 0.0), axis=1, keepdims=True)


def prep_body(
    place,
    q_hbm,
    k_hbm,
    v_hbm,
    q_gain_ref,
    k_gain_ref,
    table_hbm,
    qt_ref,
    kvt_ref,
    turned_ref,
    q_ref,
    k_ref,
    v_ref,
    table_ref,
    sems,
    *,
    heads,
    group,
):
    rows = q_ref.shape[0]
    cols = pl.ds(pl.multiple_of(place[1] * rows, rows), rows)
    copies = [
        pltpu.make_async_copy(src, dst, sems.at[i])
        for i, (src, dst) in enumerate(
            ((k_hbm, k_ref), (table_hbm.at[:, cols], table_ref), (v_hbm, v_ref), (q_hbm, q_ref))
        )
    ]
    for c in copies:
        c.start()
    for c in copies:
        c.wait()
    table = table_ref[...]
    q_gain = column(q_gain_ref[...])
    k_gain = column(k_gain_ref[...])
    qt = q_ref[...].astype(F32).T
    for h in range(heads):
        qt_ref[h * HD : (h + 1) * HD, :] = turn(qt[h * HD : (h + 1) * HD], q_gain, table, BF16)
    start = pl.multiple_of((place[0] * heads // group) * HD, HD)
    turned_ref[...] = k_ref[...].astype(F32).T
    kvt_ref[:HD, :] = turn(turned_ref[pl.ds(start, HD), :], k_gain, table, BF16)
    turned_ref[...] = v_ref[...].astype(F32).T
    kvt_ref[HD:, :] = turned_ref[pl.ds(start, HD), :].astype(BF16)


def prep(place, queries, key_input, value_input, q_gain, k_gain, table, heads):
    rows = queries.shape[0]
    return call(
        functools.partial(prep_body, heads=heads, group=HEADS // KV_HEADS),
        place,
        (queries, key_input, value_input, q_gain, k_gain, table),
        [
            hbm(),
            hbm(),
            hbm(),
            full(q_gain.shape),
            full(k_gain.shape),
            hbm(),
        ],
        [
            pltpu.HBM((queries.shape[1], rows), BF16),
            jax.ShapeDtypeStruct((2 * HD, rows), BF16),
        ],
        scratch=[
            pltpu.VMEM((key_input.shape[1], rows), F32),
            pltpu.VMEM(queries.shape, BF16),
            pltpu.VMEM(key_input.shape, BF16),
            pltpu.VMEM(value_input.shape, BF16),
            pltpu.VMEM((table.shape[0], rows), F32),
            pltpu.SemaphoreType.DMA((4,)),
        ],
        micros=2.0,
    )


def attend_body(place, qt_ref, *refs, heads, count, groups):
    sums = refs[: len(refs) - count - 4 - (groups + 1 if groups else 0)]
    refs = refs[len(sums) :]
    if groups:
        kv_refs, out_refs = refs[:count], refs[count : count + groups]
        out_ref, k_ref, v_ref, num_ref, den_ref = refs[count + groups :]
    else:
        kv_refs, (num_ref, den_ref, k_ref, v_ref) = refs[:count], refs[count:]
    num_ref[...] = sums[0][...] if sums else jnp.zeros_like(num_ref)
    den_ref[...] = sums[1][...] if sums else jnp.zeros_like(den_ref)
    keys = kv_refs[0].shape[1]
    per = kv_refs[0].shape[0] // (2 * HD)
    blocks = count * per
    for b in range(blocks):
        base = (b % per) * 2 * HD
        k_ref[b * keys : (b + 1) * keys, :] = kv_refs[b // per][base : base + HD, :].astype(F32).T.astype(BF16)
        v_ref[:, b * keys : (b + 1) * keys] = kv_refs[b // per][base + HD : base + 2 * HD, :]
    for b in range(0, blocks, SPAN):
        at = slice(b * keys, min(b + SPAN, blocks) * keys)
        for h in range(heads):
            q = qt_ref[h * HD : (h + 1) * HD, :]
            p = jnp.exp2(mm(k_ref[at, :], q) * (LOG2E * HD**-0.5))
            den_ref[h * 8 : (h + 1) * 8, :] += jnp.sum(p.reshape(p.shape[0] // 8, 8, p.shape[1]), axis=0)
            num_ref[h * HD : (h + 1) * HD, :] += mm(v_ref[:, at], p.astype(BF16))
    if groups:
        for h in range(heads):
            den = jnp.sum(den_ref[h * 8 : (h + 1) * 8, :], axis=0, keepdims=True)
            num_ref[h * HD : (h + 1) * HD, :] = num_ref[h * HD : (h + 1) * HD, :] / den
        out_ref[...] = num_ref[...].T
        rows = out_refs[0].shape[0]
        for k in range(groups):
            at = pl.multiple_of((place[0] ^ k) * rows, rows)
            out_refs[k][...] = out_ref[pl.ds(at, rows), :].astype(BF16)


def attend(place, qt, sums, kv_blocks, heads, groups):
    rows = qt.shape[1]
    keys = kv_blocks[0].shape[1]
    count = len(kv_blocks)
    total = sum(b.shape[0] for b in kv_blocks) // (2 * HD) * keys
    held = [pltpu.HBM(qt.shape, F32), pltpu.HBM((heads * 8, rows), F32)]
    scratch = [pltpu.VMEM((total, HD), BF16), pltpu.VMEM((HD, total), BF16)]
    if groups:
        outs = [jax.ShapeDtypeStruct((rows // groups, qt.shape[0]), BF16)] * groups
        scratch = [pltpu.VMEM((rows, qt.shape[0]), F32)] + scratch + [pltpu.VMEM(h.shape, F32) for h in held]
    else:
        outs = held
    return call(
        functools.partial(attend_body, heads=heads, count=count, groups=groups),
        place,
        (qt, *sums, *kv_blocks),
        [full(qt.shape)] + [full(x.shape) for x in sums] + [full(b.shape) for b in kv_blocks],
        outs,
        scratch=scratch,
        micros=16.0,
    )


def mix_body(place, *refs, groups):
    att_refs, w_refs, out_ref = refs[:groups], refs[groups : 2 * groups], refs[2 * groups]
    total = jnp.zeros(out_ref.shape, F32)
    for k in range(groups):
        total += mm(att_refs[k][...], w_refs[k][...]).astype(BF16).astype(F32)
    out_ref[...] = total.astype(BF16)


def mix(place, atts, weights):
    groups = len(weights)
    rows = atts[0].shape[0]
    depth, width = weights[0].shape
    tile = min(width, 512)
    return call(
        functools.partial(mix_body, groups=groups),
        place,
        (*atts, *weights),
        [full(a.shape) for a in atts] + [pl.BlockSpec((depth, tile), lambda j, place: (0, j))] * groups,
        [jax.ShapeDtypeStruct((rows, width), BF16)],
        grid=(width // tile,),
        out_specs=[pl.BlockSpec((rows, tile), lambda j, place: (0, j))],
        micros=2.5,
    )[0]


def expert_body(place, *refs, groups, tile, experts):
    x_refs = refs[:groups]
    gain_ref, gate_ref, up_ref, down_ref = refs[groups : groups + 4]
    out_refs = refs[groups + 4 : 3 * groups + 4]
    scaled_ref, hidden_ref = refs[3 * groups + 4 :]
    rows, feat = x_refs[0].shape
    cap = rows // experts
    half = rows // 2
    width = groups * feat

    def spot(k):
        return pl.ds(pl.multiple_of((place[0] ^ k) * feat, feat), feat)

    parts = []
    for i in range(experts):
        at = pl.multiple_of((place[1] ^ i ^ (experts // 2)) * cap, cap)
        squares = 0.0
        for k in range(groups):
            x = x_refs[k][pl.ds(at, cap), :].astype(F32)
            scaled_ref[i * cap : (i + 1) * cap, spot(k)] = (x * gain_ref[:, spot(k)]).astype(BF16)
            squares += x * x
        parts.append(jnp.sum(squares, axis=1, keepdims=True))
    scale = lax.rsqrt(jnp.concatenate(parts, axis=0) / width + EPSILON)

    for j in range(gate_ref.shape[1] // tile):
        x = scaled_ref[...]
        cols = slice(j * tile, (j + 1) * tile)
        gate = mm(x, gate_ref[:, cols]) * scale
        up = mm(x, up_ref[:, cols]) * scale
        hidden_ref[:, cols] = (gate / (1.0 + jnp.exp(-gate)) * up).astype(BF16)
    for k in range(groups):
        part = mm(hidden_ref[...], down_ref[:, spot(k)]).astype(BF16)
        out_refs[2 * k][...] = part[:half]
        out_refs[2 * k + 1][...] = part[half:]


def expert(place, xs, gain, gate, up, down, experts):
    groups = len(xs)
    rows, feat = xs[0].shape
    depth, ff = gate.shape
    tile = min(ff, 256)
    vmem = pl.BlockSpec(memory_space=pltpu.VMEM)
    return call(
        functools.partial(expert_body, groups=groups, tile=tile, experts=experts),
        place,
        (*xs, gain, gate, up, down),
        [full(x.shape) for x in xs] + [full(gain.shape), vmem, vmem, vmem],
        [jax.ShapeDtypeStruct((rows // 2, feat), BF16)] * (2 * groups),
        scratch=[pltpu.VMEM((rows, depth), BF16), pltpu.VMEM((rows, ff), BF16)],
        micros=9.0,
    )


def combine_body(place, slot_ref, scores_ref, *refs, blocks):
    out_ref, rows_ref = refs[blocks:]
    tokens = out_ref.shape[0]
    cap = refs[0].shape[0]
    for i in range(blocks):
        rows_ref[i * cap : (i + 1) * cap, :] = refs[i][...]
    scores = scores_ref[...]
    weight = scores / jnp.sum(scores, axis=0, keepdims=True)
    slot = slot_ref[...]
    rows = lax.broadcasted_iota(jnp.int32, (blocks * cap, tokens), 0)
    total = jnp.zeros(out_ref.shape, F32)
    for k in range(2):
        pick = (rows == slot[k : k + 1, :]).astype(F32).astype(BF16)
        total += mm(pick, rows_ref[...], ((0,), (0,))) * column(weight[k : k + 1, :])
    out_ref[...] = total.astype(BF16)


def combine(place, slot, scores, rows):
    cap, feat = rows[0].shape
    return call(
        functools.partial(combine_body, blocks=len(rows)),
        place,
        (slot, scores, *rows),
        [full(slot.shape), full(scores.shape)] + [full(r.shape) for r in rows],
        [jax.ShapeDtypeStruct((slot.shape[1], feat), BF16)],
        scratch=[pltpu.VMEM((len(rows) * cap, feat), BF16)],
        micros=1.5,
    )[0]


def local(
    table,
    queries,
    key_input,
    value_input,
    query_gain,
    key_gain,
    mix_out_weight,
    expert_input,
    ffn_gain,
    routes,
    route_scores,
    gate_weight,
    up_weight,
    down_weight,
):
    n_ep = lax.axis_size("ep")
    n_tp = lax.axis_size("tp")
    heads = queries.shape[1] // HD
    tokens, top = routes.shape
    width = expert_input.shape[1]
    feat = width // n_tp
    cap = 3 * tokens * top // (2 * n_ep)
    cap = -(-cap // 8) * 8
    place = jnp.stack([lax.axis_index("tp"), lax.axis_index("ep")]).astype(jnp.int32)
    half = n_ep // 2

    weights = {0: mix_out_weight}
    for k in range(2, n_tp, 2):
        weights[k] = send(mix_out_weight, "tp", k)
    for k in range(0, n_tp, 2):
        weights[k + 1] = send(weights[k], "tp", 1)

    qt, kvt = prep(
        place,
        *map(far_memory, (queries, key_input, value_input, query_gain[None], key_gain[None], table)),
        heads,
    )
    pair = jnp.concatenate([kvt, send(kvt, "ep", 1)], axis=0)
    along = [send(pair, "ep", k) for k in range(n_ep - 2, 0, -2)]

    outbound, slot = dispatch(place, far_memory(routes.T), far_memory(expert_input), n_ep, cap, feat)
    arrived = lax.all_to_all(outbound, "ep", split_axis=0, concat_axis=0, tiled=True)
    xs = {0: arrived}
    for k in range(2, n_tp, 2):
        xs[k] = send(arrived, "tp", k)
    for k in range(0, n_tp, 2):
        xs[k + 1] = send(xs[k], "tp", 1)

    qt = far_memory(qt)
    sums = attend(place, qt, (), [pair], heads, 0)
    atts = attend(place, qt, [far_memory(x) for x in sums], along, heads, n_tp)
    atts = [atts[0]] + [send(atts[k], "tp", k) for k in range(1, n_tp)]

    parts = expert(
        place, [xs[k] for k in range(n_tp)], far_memory(ffn_gain[None]), gate_weight[0], up_weight[0], down_weight[0], n_ep
    )
    returned = []
    for side in range(2):
        mine = {k: (parts[2 * k + side], send(parts[2 * k + 2 + side], "tp", 1)) for k in range(0, n_tp, 2)}
        terms = list(mine[0])
        for k in range(2, n_tp, 2):
            both = (mine[k][0].astype(F32) + mine[k][1].astype(F32)).astype(BF16)
            terms.append(send(both, "tp", k))
        for i in range(half):
            piece = sum(t[i * cap : (i + 1) * cap].astype(F32) for t in terms).astype(BF16)
            k = i ^ half if side == 0 else i
            returned.append(send(piece, "ep", k) if k else piece)

    mixed = mix(place, atts, [weights[k] for k in range(n_tp)])
    out = combine(place, slot, route_scores.T, returned)
    return mixed, out


def solution(mesh):
    n_ep = mesh.shape["ep"]
    placed = (
        P(),
        P("ep", "tp"),
        P("ep", None),
        P("ep", None),
        P(),
        P(),
        P("tp", None),
        P("ep", None),
        P(),
        P("ep", None),
        P("ep", None),
        P("ep", None, "tp"),
        P("ep", None, "tp"),
        P("ep", "tp", None),
    )

    step = jax.shard_map(
        local,
        mesh=mesh,
        in_specs=placed,
        out_specs=(P(("ep", "tp"), None), P("ep", "tp")),
        check_vma=False,
    )

    def run(queries, *rest):
        table = jnp.asarray(rope_tables(queries.shape[0] // n_ep, n_ep))
        return step(table, queries, *rest)

    return run
```

```python
import functools

import jax
import jax.numpy as jnp
import numpy as np
from jax import lax
from jax.experimental import pallas as pl
from jax.experimental.pallas import tpu as pltpu
from jax.sharding import PartitionSpec as P


HEADS = 16
KV_HEADS = 4
HD = 64
GRID_W = 64
EPSILON = 1e-06
ROPE_BASE = 10000.0
LOG2E = 1.4426950408889634
F32 = jnp.float32
BF16 = jnp.bfloat16
VMEM_LIMIT = 24 * 1024 * 1024
FLOPS_PER_MICRO = 500_000_000
SPAN = 6


def full(shape):
    return pl.BlockSpec(shape, lambda *_: (0,) * len(shape))


def hbm():
    return pl.BlockSpec(memory_space=pltpu.HBM)


def far_memory(x):
    return pltpu.with_memory_space_constraint(x, pltpu.HBM)


def call(body, place, args, in_specs, outs, grid=(1,), scratch=(), out_specs=None, micros=1.0):
    return pl.pallas_call(
        body,
        grid_spec=pltpu.PrefetchScalarGridSpec(
            num_scalar_prefetch=1,
            grid=grid,
            in_specs=in_specs,
            out_specs=[full(o.shape) for o in outs] if out_specs is None else out_specs,
            scratch_shapes=list(scratch),
        ),
        out_shape=outs,
        cost_estimate=pl.CostEstimate(
            flops=int(micros * FLOPS_PER_MICRO), transcendentals=0, bytes_accessed=0
        ),
        compiler_params=pltpu.CompilerParams(
            dimension_semantics=("arbitrary",) * len(grid), vmem_limit_bytes=VMEM_LIMIT
        ),
    )(place, *args)


def mm(a, b, dims=((1,), (0,))):
    return lax.dot_general(a, b, (dims, ((), ())), preferred_element_type=F32)


def send(x, axis, flip):
    n = lax.axis_size(axis)
    return lax.ppermute(x, axis, [(i, i ^ flip) for i in range(n)])


def dispatch_body(place, routes_hbm, x_hbm, out_ref, slot_ref, x_ref, routes_ref, sem, routes_sem, *, experts, cap):
    tokens, feat = x_ref.shape
    cols = pl.ds(pl.multiple_of(place[0] * feat, feat), feat)
    fetch = pltpu.make_async_copy(x_hbm.at[:, cols], x_ref, sem)
    fetch_routes = pltpu.make_async_copy(routes_hbm, routes_ref, routes_sem)
    fetch_routes.start()
    fetch.start()
    fetch_routes.wait()
    routes = routes_ref[...]
    rows = lax.broadcasted_iota(jnp.int32, (experts, tokens), 0)
    first = (rows == routes[0:1, :]).astype(F32)
    second = (rows == routes[1:2, :]).astype(F32)
    hits = first + second
    row = lax.broadcasted_iota(jnp.int32, (tokens, tokens), 0)
    col = lax.broadcasted_iota(jnp.int32, (tokens, tokens), 1)
    before = (row < col).astype(F32).astype(BF16)
    count = mm(hits.astype(BF16), before)
    slot = jnp.where(hits > 0.5, count, -1.0).astype(jnp.int32)

    def flat(choice, expert):
        at = jnp.sum(count * choice, axis=0, keepdims=True).astype(jnp.int32)
        return (expert ^ place[1] ^ (experts // 2)) * cap + at

    slot_ref[0:1, :] = flat(first, routes[0:1, :])
    slot_ref[1:2, :] = flat(second, routes[1:2, :])
    fetch.wait()
    x = x_ref[...]
    slots = lax.broadcasted_iota(jnp.int32, (cap, tokens), 0)
    picks = [(slots == slot[e : e + 1, :]).astype(F32) for e in range(experts)]
    out_ref[...] = mm(jnp.concatenate(picks, axis=0).astype(BF16), x).astype(BF16)


def dispatch(place, routes, expert_input, experts, cap, feat):
    tokens = routes.shape[1]
    outs = [jax.ShapeDtypeStruct((experts * cap, feat), BF16), jax.ShapeDtypeStruct((2, tokens), jnp.int32)]
    return call(
        functools.partial(dispatch_body, experts=experts, cap=cap),
        place,
        (routes, expert_input),
        [hbm(), hbm()],
        outs,
        scratch=[
            pltpu.VMEM((tokens, feat), BF16),
            pltpu.VMEM(routes.shape, jnp.int32),
            pltpu.SemaphoreType.DMA,
            pltpu.SemaphoreType.DMA,
        ],
        micros=1.5,
    )


def rope_tables(token_count, n_ep):
    quarter = HD // 4
    inverse = (np.float32(ROPE_BASE) ** (-np.arange(quarter, dtype=np.float32) / np.float32(quarter))).astype(
        np.float32
    )
    pos = np.arange(token_count * n_ep)

    def both(steps):
        angle = (inverse[:, None] * steps.astype(np.float32)[None, :]).astype(np.float32).astype(np.float64)
        return np.concatenate([np.cos(angle), np.sin(angle)], 0).astype(np.float32)

    return np.concatenate([both(pos // GRID_W), both(pos % GRID_W)], 0)


def turn(x, gain, table, low):
    quarter = HD // 4
    x = x.astype(F32)
    scale = lax.rsqrt(jnp.mean(x * x, axis=0, keepdims=True) + EPSILON)
    x = x * scale * gain
    u0, w0, u1, w1 = (x[i * quarter : (i + 1) * quarter] for i in range(4))
    cr, sr, cc, sc = (table[i * quarter : (i + 1) * quarter] for i in range(4))
    return jnp.concatenate(
        [u0 * cr - w0 * sr, w0 * cr + u0 * sr, u1 * cc - w1 * sc, w1 * cc + u1 * sc], axis=0
    ).astype(low)


def column(row):
    n = row.shape[1]
    same = lax.broadcasted_iota(jnp.int32, (n, n), 0) == lax.broadcasted_iota(jnp.int32, (n, n), 1)
    return jnp.sum(jnp.where(same, row, 0.0), axis=1, keepdims=True)


def prep_body(
    place,
    q_hbm,
    k_hbm,
    v_hbm,
    q_gain_ref,
    k_gain_ref,
    table_hbm,
    qt_ref,
    kvt_ref,
    turned_ref,
    q_ref,
    k_ref,
    v_ref,
    table_ref,
    sems,
    *,
    heads,
    group,
):
    rows = q_ref.shape[0]
    cols = pl.ds(pl.multiple_of(place[1] * rows, rows), rows)
    copies = [
        pltpu.make_async_copy(src, dst, sems.at[i])
        for i, (src, dst) in enumerate(
            ((k_hbm, k_ref), (table_hbm.at[:, cols], table_ref), (v_hbm, v_ref), (q_hbm, q_ref))
        )
    ]
    for c in copies:
        c.start()
    for c in copies:
        c.wait()
    table = table_ref[...]
    q_gain = column(q_gain_ref[...])
    k_gain = column(k_gain_ref[...])
    qt = q_ref[...].astype(F32).T
    for h in range(heads):
        qt_ref[h * HD : (h + 1) * HD, :] = turn(qt[h * HD : (h + 1) * HD], q_gain, table, BF16)
    start = pl.multiple_of((place[0] * heads // group) * HD, HD)
    turned_ref[...] = k_ref[...].astype(F32).T
    kvt_ref[:HD, :] = turn(turned_ref[pl.ds(start, HD), :], k_gain, table, BF16)
    turned_ref[...] = v_ref[...].astype(F32).T
    kvt_ref[HD:, :] = turned_ref[pl.ds(start, HD), :].astype(BF16)


def prep(place, queries, key_input, value_input, q_gain, k_gain, table, heads):
    rows = queries.shape[0]
    return call(
        functools.partial(prep_body, heads=heads, group=HEADS // KV_HEADS),
        place,
        (queries, key_input, value_input, q_gain, k_gain, table),
        [
            hbm(),
            hbm(),
            hbm(),
            full(q_gain.shape),
            full(k_gain.shape),
            hbm(),
        ],
        [
            pltpu.HBM((queries.shape[1], rows), BF16),
            jax.ShapeDtypeStruct((2 * HD, rows), BF16),
        ],
        scratch=[
            pltpu.VMEM((key_input.shape[1], rows), F32),
            pltpu.VMEM(queries.shape, BF16),
            pltpu.VMEM(key_input.shape, BF16),
            pltpu.VMEM(value_input.shape, BF16),
            pltpu.VMEM((table.shape[0], rows), F32),
            pltpu.SemaphoreType.DMA((4,)),
        ],
        micros=2.0,
    )


def attend_body(place, qt_ref, *refs, heads, count, groups):
    sums = refs[: len(refs) - count - 4 - (groups + 1 if groups else 0)]
    refs = refs[len(sums) :]
    if groups:
        kv_refs, out_refs = refs[:count], refs[count : count + groups]
        out_ref, k_ref, v_ref, num_ref, den_ref = refs[count + groups :]
    else:
        kv_refs, (num_ref, den_ref, k_ref, v_ref) = refs[:count], refs[count:]
    num_ref[...] = sums[0][...] if sums else jnp.zeros_like(num_ref)
    den_ref[...] = sums[1][...] if sums else jnp.zeros_like(den_ref)
    keys = kv_refs[0].shape[1]
    per = kv_refs[0].shape[0] // (2 * HD)
    blocks = count * per
    for b in range(blocks):
        base = (b % per) * 2 * HD
        k_ref[b * keys : (b + 1) * keys, :] = kv_refs[b // per][base : base + HD, :].astype(F32).T.astype(BF16)
        v_ref[:, b * keys : (b + 1) * keys] = kv_refs[b // per][base + HD : base + 2 * HD, :]
    for b in range(0, blocks, SPAN):
        at = slice(b * keys, min(b + SPAN, blocks) * keys)
        for h in range(heads):
            q = qt_ref[h * HD : (h + 1) * HD, :]
            p = jnp.exp2(mm(k_ref[at, :], q) * (LOG2E * HD**-0.5))
            den_ref[h * 8 : (h + 1) * 8, :] += jnp.sum(p.reshape(p.shape[0] // 8, 8, p.shape[1]), axis=0)
            num_ref[h * HD : (h + 1) * HD, :] += mm(v_ref[:, at], p.astype(BF16))
    if groups:
        for h in range(heads):
            den = jnp.sum(den_ref[h * 8 : (h + 1) * 8, :], axis=0, keepdims=True)
            num_ref[h * HD : (h + 1) * HD, :] = num_ref[h * HD : (h + 1) * HD, :] / den
        out_ref[...] = num_ref[...].T
        rows = out_refs[0].shape[0]
        for k in range(groups):
            at = pl.multiple_of((place[0] ^ k) * rows, rows)
            out_refs[k][...] = out_ref[pl.ds(at, rows), :].astype(BF16)


def attend(place, qt, sums, kv_blocks, heads, groups):
    rows = qt.shape[1]
    keys = kv_blocks[0].shape[1]
    count = len(kv_blocks)
    total = sum(b.shape[0] for b in kv_blocks) // (2 * HD) * keys
    held = [pltpu.HBM(qt.shape, F32), pltpu.HBM((heads * 8, rows), F32)]
    scratch = [pltpu.VMEM((total, HD), BF16), pltpu.VMEM((HD, total), BF16)]
    if groups:
        outs = [jax.ShapeDtypeStruct((rows // groups, qt.shape[0]), BF16)] * groups
        scratch = [pltpu.VMEM((rows, qt.shape[0]), F32)] + scratch + [pltpu.VMEM(h.shape, F32) for h in held]
    else:
        outs = held
    return call(
        functools.partial(attend_body, heads=heads, count=count, groups=groups),
        place,
        (qt, *sums, *kv_blocks),
        [full(qt.shape)] + [full(x.shape) for x in sums] + [full(b.shape) for b in kv_blocks],
        outs,
        scratch=scratch,
        micros=16.0,
    )


def mix_body(place, *refs, groups):
    att_refs, w_refs, out_ref = refs[:groups], refs[groups : 2 * groups], refs[2 * groups]
    width = out_ref.shape[1]
    tile = min(width, 1024)
    for j in range(0, width, tile):
        total = 0.0
        for k in range(groups):
            total += mm(att_refs[k][...], w_refs[k][:, j : j + tile]).astype(BF16).astype(F32)
        out_ref[:, j : j + tile] = total.astype(BF16)


def mix(place, atts, weights):
    groups = len(weights)
    rows = atts[0].shape[0]
    return call(
        functools.partial(mix_body, groups=groups),
        place,
        (*atts, *weights),
        [full(a.shape) for a in atts] + [full(w.shape) for w in weights],
        [jax.ShapeDtypeStruct((rows, weights[0].shape[1]), BF16)],
        micros=2.5,
    )[0]


def expert_body(place, *refs, groups, tile, experts):
    x_refs = refs[:groups]
    gain_ref, gate_ref, up_ref, down_ref = refs[groups : groups + 4]
    out_refs = refs[groups + 4 : 3 * groups + 4]
    scaled_ref, hidden_ref = refs[3 * groups + 4 :]
    rows, feat = x_refs[0].shape
    cap = rows // experts
    half = rows // 2
    width = groups * feat

    def spot(k):
        return pl.ds(pl.multiple_of((place[0] ^ k) * feat, feat), feat)

    parts = []
    for i in range(experts):
        at = pl.multiple_of((place[1] ^ i ^ (experts // 2)) * cap, cap)
        squares = 0.0
        for k in range(groups):
            x = x_refs[k][pl.ds(at, cap), :].astype(F32)
            scaled_ref[i * cap : (i + 1) * cap, spot(k)] = (x * gain_ref[:, spot(k)]).astype(BF16)
            squares += x * x
        parts.append(jnp.sum(squares, axis=1, keepdims=True))
    scale = lax.rsqrt(jnp.concatenate(parts, axis=0) / width + EPSILON)

    for j in range(gate_ref.shape[1] // tile):
        x = scaled_ref[...]
        cols = slice(j * tile, (j + 1) * tile)
        gate = mm(x, gate_ref[:, cols]) * scale
        up = mm(x, up_ref[:, cols]) * scale
        hidden_ref[:, cols] = (gate / (1.0 + jnp.exp(-gate)) * up).astype(BF16)
    for k in range(groups):
        part = mm(hidden_ref[...], down_ref[:, spot(k)]).astype(BF16)
        out_refs[2 * k][...] = part[:half]
        out_refs[2 * k + 1][...] = part[half:]


def expert(place, xs, gain, gate, up, down, experts):
    groups = len(xs)
    rows, feat = xs[0].shape
    depth, ff = gate.shape
    tile = min(ff, 256)
    vmem = pl.BlockSpec(memory_space=pltpu.VMEM)
    return call(
        functools.partial(expert_body, groups=groups, tile=tile, experts=experts),
        place,
        (*xs, gain, gate, up, down),
        [full(x.shape) for x in xs] + [full(gain.shape), vmem, vmem, vmem],
        [jax.ShapeDtypeStruct((rows // 2, feat), BF16)] * (2 * groups),
        scratch=[pltpu.VMEM((rows, depth), BF16), pltpu.VMEM((rows, ff), BF16)],
        micros=9.0,
    )


def combine_body(place, slot_ref, scores_ref, *refs, blocks):
    out_ref, rows_ref = refs[blocks:]
    tokens = out_ref.shape[0]
    cap = refs[0].shape[0]
    for i in range(blocks):
        rows_ref[i * cap : (i + 1) * cap, :] = refs[i][...]
    scores = scores_ref[...]
    weight = scores / jnp.sum(scores, axis=0, keepdims=True)
    slot = slot_ref[...]
    rows = lax.broadcasted_iota(jnp.int32, (blocks * cap, tokens), 0)
    total = jnp.zeros(out_ref.shape, F32)
    for k in range(2):
        pick = (rows == slot[k : k + 1, :]).astype(F32).astype(BF16)
        total += mm(pick, rows_ref[...], ((0,), (0,))) * column(weight[k : k + 1, :])
    out_ref[...] = total.astype(BF16)


def combine(place, slot, scores, rows):
    cap, feat = rows[0].shape
    return call(
        functools.partial(combine_body, blocks=len(rows)),
        place,
        (slot, scores, *rows),
        [full(slot.shape), full(scores.shape)] + [full(r.shape) for r in rows],
        [jax.ShapeDtypeStruct((slot.shape[1], feat), BF16)],
        scratch=[pltpu.VMEM((len(rows) * cap, feat), BF16)],
        micros=1.5,
    )[0]


def local(
    table,
    queries,
    key_input,
    value_input,
    query_gain,
    key_gain,
    mix_out_weight,
    expert_input,
    ffn_gain,
    routes,
    route_scores,
    gate_weight,
    up_weight,
    down_weight,
):
    n_ep = lax.axis_size("ep")
    n_tp = lax.axis_size("tp")
    heads = queries.shape[1] // HD
    tokens, top = routes.shape
    width = expert_input.shape[1]
    feat = width // n_tp
    cap = 3 * tokens * top // (2 * n_ep)
    cap = -(-cap // 8) * 8
    place = jnp.stack([lax.axis_index("tp"), lax.axis_index("ep")]).astype(jnp.int32)
    half = n_ep // 2

    weights = {0: mix_out_weight}
    for k in range(2, n_tp, 2):
        weights[k] = send(mix_out_weight, "tp", k)
    for k in range(0, n_tp, 2):
        weights[k + 1] = send(weights[k], "tp", 1)

    qt, kvt = prep(
        place,
        *map(far_memory, (queries, key_input, value_input, query_gain[None], key_gain[None], table)),
        heads,
    )
    pair = jnp.concatenate([kvt, send(kvt, "ep", 1)], axis=0)
    along = [send(pair, "ep", k) for k in range(n_ep - 2, 0, -2)]

    outbound, slot = dispatch(place, far_memory(routes.T), far_memory(expert_input), n_ep, cap, feat)
    arrived = lax.all_to_all(outbound, "ep", split_axis=0, concat_axis=0, tiled=True)
    xs = {0: arrived}
    for k in range(2, n_tp, 2):
        xs[k] = send(arrived, "tp", k)
    for k in range(0, n_tp, 2):
        xs[k + 1] = send(xs[k], "tp", 1)

    qt = far_memory(qt)
    sums = attend(place, qt, (), [pair], heads, 0)
    atts = attend(place, qt, [far_memory(x) for x in sums], along, heads, n_tp)
    atts = [atts[0]] + [send(atts[k], "tp", k) for k in range(1, n_tp)]

    parts = expert(
        place, [xs[k] for k in range(n_tp)], far_memory(ffn_gain[None]), gate_weight[0], up_weight[0], down_weight[0], n_ep
    )
    returned = []
    for side in range(2):
        mine = {k: (parts[2 * k + side], send(parts[2 * k + 2 + side], "tp", 1)) for k in range(0, n_tp, 2)}
        terms = list(mine[0])
        for k in range(2, n_tp, 2):
            both = (mine[k][0].astype(F32) + mine[k][1].astype(F32)).astype(BF16)
            terms.append(send(both, "tp", k))
        for i in range(half):
            piece = sum(t[i * cap : (i + 1) * cap].astype(F32) for t in terms).astype(BF16)
            k = i ^ half if side == 0 else i
            returned.append(send(piece, "ep", k) if k else piece)

    mixed = mix(place, atts, [weights[k] for k in range(n_tp)])
    out = combine(place, slot, route_scores.T, returned)
    return mixed, out


def solution(mesh):
    n_ep = mesh.shape["ep"]
    placed = (
        P(),
        P("ep", "tp"),
        P("ep", None),
        P("ep", None),
        P(),
        P(),
        P("tp", None),
        P("ep", None),
        P(),
        P("ep", None),
        P("ep", None),
        P("ep", None, "tp"),
        P("ep", None, "tp"),
        P("ep", "tp", None),
    )

    step = jax.shard_map(
        local,
        mesh=mesh,
        in_specs=placed,
        out_specs=(P(("ep", "tp"), None), P("ep", "tp")),
        check_vma=False,
    )

    def run(queries, *rest):
        table = jnp.asarray(rope_tables(queries.shape[0] // n_ep, n_ep))
        return step(table, queries, *rest)

    return run
```
